32 devices in a mesh: grp: 2 (over y), sp: 4 (over z), tp: 4 (over x, core).
Axes of the slice: x: 2, y: 2, z: 4, core: 2. Of those that a mesh axis runs over, the one named last changes fastest.
Arguments:
- recept: bfloat16 [4096, 2048], P(('grp', 'sp'), 'tp'), parts along dimension 0, may hold values from -6 to 6
- key_input: bfloat16 [4096, 2048], P(('grp', 'sp'), 'tp'), parts along dimension 0, may hold values from -6 to 6
- value_input: bfloat16 [4096, 2048], P(('grp', 'sp'), 'tp'), parts along dimension 0, may hold values from -6 to 6
- output_gate_input: bfloat16 [4096, 2048], P(('grp', 'sp'), 'tp'), parts along dimension 0, may hold values from -6 to 6
- decay_input_part: bfloat16 [4096, 2048], P(('grp', 'sp'), 'tp'), parts along dimension 0, may hold values from -4.8 to 4.8
- correction_rate_input: bfloat16 [4096, 2048], P(('grp', 'sp'), 'tp'), parts along dimension 0, may hold values from -4 to 4
- head_decay_offset: float32 [4096, 32], P(('grp', 'sp'), 'tp'), parts along dimension 0, may hold values from -2.1 to 0
- decay_fixed_bias: float32 [2048], P('tp'), may hold values from -11.5 to -2.8
- correction_rate_bias: float32 [2048], P('tp'), may hold values from -8.5 to 1
- head_norm_gain: float32 [2048], P('tp'), may hold values from 0.1 to 1.9
- self_term_weight: float32 [2048], P('tp'), may hold values from -2 to 2
- output_weight_matrix: bfloat16 [2048, 2048], P('tp'), may hold values from -0.125 to 0.125
- residual: bfloat16 [4096, 2048], P(('grp', 'sp', 'tp')), parts along dimension 0, may hold values from -6 to 6
- feedforward_norm_gain: float32 [2048], replicated, may hold values from 0.1 to 1.9
- routed_expert_index: int32 [4096, 2], P(('grp', 'sp', 'tp')), parts along dimension 0, may hold values from 0 to 3, all different within a row; in each aligned block of 128 rows (0 to 127, 128 to 255, ...) at most 96 rows name the same one
- routed_expert_weight: float32 [4096, 2], P(('grp', 'sp', 'tp')), parts along dimension 0, may hold values from 0.2 to 1
- gate_weight_experts: bfloat16 [4, 2048, 1024], P('sp', None, 'tp'), may hold values from -0.125 to 0.125
- up_weight_experts: bfloat16 [4, 2048, 1024], P('sp', None, 'tp'), may hold values from -0.125 to 0.125
- down_weight_experts: bfloat16 [4, 1024, 2048], P('sp', 'tp'), may hold values from -0.1875 to 0.1875
Outputs:
- output: bfloat16 [4096, 2048], P(('grp', 'sp', 'tp')), parts along dimension 0
The draws below stay inside these ranges and needn't reach their ends.
There are 2 independent parts, one for each index of `grp`. The reference program is written for one: setup_inputs(seed, part) draws one part's arguments, and reference() takes and returns one part's arrays. A program takes and returns all parts, laid end to end along the dimension named above; an argument that names none is the same for every part. Nothing has to cross between parts.
Inputs may be any that keep to these rules, and one draw needn't show every extreme that they name: `routed_expert_index`: in each aligned block of 128 rows (the rows of one device) no expert is named by more than 96 routes; the two experts of a row differ.
All inputs are finite; a program needn't handle non-finite values.
Results may differ from the reference program's by a relative error of at most 0.0058.
Values may be sent and summed in bfloat16 or wider, within the bound.
A program may use at most 128 MiB of HBM per device.

```python
import math
import jax
import jax.numpy as jnp
import numpy as np
from jax import lax

D = 2048
HEAD_COUNT = 32
HEAD_CHANNELS = 64
MODEL_WIDTH = 2048
FF = 1024
EXPERTS = 4
TOK_SP = 512
SEQUENCE_TOKENS = 2048
CAP = 96
N_SP = 4
N_TP = 4


def head_kinds(key):
    share = 5
    fast_heads = jax.random.randint(jax.random.fold_in(key, 11), (HEAD_COUNT,), 0, 10) < share
    return jnp.repeat(fast_heads, HEAD_CHANNELS)


def draw_decay_fixed_bias(key, part):
    fast_chan = head_kinds(key)
    uniform_draw = jax.random.uniform(jax.random.fold_in(key, 12), (MODEL_WIDTH,), jnp.float32)
    return jnp.where(fast_chan, -3.8 + uniform_draw, -11.5 + uniform_draw).astype(jnp.float32)


def draw_correction_rate_bias(key, part):
    fast_chan = head_kinds(key)
    uniform_draw = jax.random.uniform(jax.random.fold_in(key, 13), (MODEL_WIDTH,), jnp.float32)
    return jnp.where(fast_chan, -1.0 + 2.0 * uniform_draw, -8.5 + uniform_draw).astype(jnp.float32)


def draw_decay_input_part(key, part):
    noise = jnp.clip(jax.random.normal(jax.random.fold_in(key, 21), (SEQUENCE_TOKENS, MODEL_WIDTH), jnp.float32), -4.0, 4.0)
    shifts = jax.random.uniform(jax.random.fold_in(key, 22), (SEQUENCE_TOKENS // TOK_SP, 1, 1), jnp.float32, -0.8, 0.8)
    shaped = noise.reshape(SEQUENCE_TOKENS // TOK_SP, TOK_SP, MODEL_WIDTH) + shifts
    return shaped.reshape(SEQUENCE_TOKENS, MODEL_WIDTH).astype(jnp.bfloat16)


def draw_correction_rate_input(key, part):
    noise = jnp.clip(jax.random.normal(jax.random.fold_in(key, 31), (SEQUENCE_TOKENS, MODEL_WIDTH), jnp.float32), -4.0, 4.0)
    return noise.astype(jnp.bfloat16)


def draw_head_decay_offset(key, part):
    spots = jax.random.randint(jax.random.fold_in(key, 41), (3, HEAD_COUNT), 0, SEQUENCE_TOKENS)
    losses = jnp.log(jax.random.uniform(jax.random.fold_in(key, 42), (3, HEAD_COUNT), jnp.float32, 0.5, 0.8))
    places = jnp.arange(SEQUENCE_TOKENS, dtype=jnp.int32)[None, :, None]
    hits = places == spots[:, None, :]
    return jnp.sum(jnp.where(hits, losses[:, None, :], 0.0), axis=0).astype(jnp.float32)


def level_of(rng, dims, split, least, top_value):
    gain, own = 1.0, jax.random.fold_in(rng, 6)
    for dim, blocks in split:
        draws = jnp.exp(jax.random.uniform(jax.random.fold_in(own, dim), (blocks,), jnp.float32, least / len(split), top_value / len(split)))
        gain = gain * jnp.repeat(draws, dims[dim] // blocks).reshape([-1 if axis == dim else 1 for axis in range(len(dims))])
    return gain


def routed_block(rng, own, number, rows, amount, top, most, lean):
    sequence = jax.random.permutation(rng, amount)
    crowded, common = load_shares(amount, rows * top, most, lean, True), load_shares(amount, rows * top, most, lean, False)
    places = jnp.arange(amount)

    def named(sizes, turn):
        used = int((sizes > 0).sum())
        fixed = max(1, used // 4)
        moved = fixed + (places - fixed + turn * (used - fixed)) % max(1, amount - fixed)
        return jnp.zeros((amount,), jnp.int32).at[sequence[jnp.where(places < fixed, places, moved)]].set(jnp.asarray(sizes, jnp.int32))

    sizes = jnp.where(number % 4 == 0, named(crowded, number // 4), named(common, number - number // 4 - 1))
    mixed = jax.random.permutation(jax.random.fold_in(own, 3), amount)
    donor, receiver = mixed[0:amount // 2 * 2:2], mixed[1:amount // 2 * 2:2]
    slack = jnp.minimum(sizes[donor] - 1, most - sizes[receiver]) // 2
    slack = jnp.where((donor == sequence[0]) | (receiver == sequence[0]) | (sizes[receiver] == 0), 0, jnp.maximum(slack, 0))
    moved = jax.random.randint(jax.random.fold_in(own, 4), (amount // 2,), 0, 1 << 20) % (slack + 1)
    sizes = sizes.at[donor].add(-moved).at[receiver].add(moved)
    labels = jnp.searchsorted(jnp.cumsum(sizes), jnp.arange(rows * top), side="right").astype(jnp.int32)
    table = labels.reshape(top, rows).T
    table = table[jax.random.permutation(jax.random.fold_in(own, 1), rows)]
    turn = jax.random.randint(jax.random.fold_in(own, 2), (rows, 1), 0, top)
    return jnp.take_along_axis(table, (jnp.arange(top)[None, :] + turn) % top, axis=1)


def load_shares(count, total, limit, slope, full):
    portions = [(1 << 20) // math.isqrt(rank ** slope) + 1 for rank in range(1, count + 1)]
    largest = limit if full else min(limit, max(-(-total // count), total * portions[0] // sum(portions)))
    least = 1 if total - largest >= count - 1 else 0
    given, surplus = [largest] + [least] * (count - 1), total - largest - least * (count - 1)
    while surplus > 0:
        candidates = [i for i in range(1, count) if given[i] < largest] or [i for i in range(1, count) if given[i] < limit]
        whole, remaining = sum([portions[i] for i in candidates]), surplus
        for i in candidates:
            extra = min(limit - given[i], max(1, remaining * portions[i] // whole), surplus)
            given[i] = given[i] + extra
            surplus = surplus - extra
    return np.array(given)


def bell_draw(stream_key, dims, width, reach, shards=(), held_as=jnp.bfloat16):
    values = jax.random.normal(stream_key, dims, jnp.float32) * width
    if len(shards) > 0:
        values = level_of(stream_key, dims, shards, -0.22, 0.18) * values
    return jnp.clip(values, min=-reach, max=reach).astype(held_as)


def setup_inputs(seed: int = 0, part: int = 0) -> dict:
    streams_of = jax.random.split(jax.random.key(seed), 20)
    own_keys = jax.random.split(jax.random.fold_in(streams_of[19], part), 20)
    recept = bell_draw(own_keys[0], (SEQUENCE_TOKENS, MODEL_WIDTH), 1.0, 6.0, ((0, 4), (1, 4)))
    key_input = bell_draw(own_keys[1], (SEQUENCE_TOKENS, MODEL_WIDTH), 1.0, 6.0, ((0, 4), (1, 4)))
    value_input = bell_draw(own_keys[2], (SEQUENCE_TOKENS, MODEL_WIDTH), 1.0, 6.0, ((0, 4), (1, 4)))
    output_gate_input = bell_draw(own_keys[3], (SEQUENCE_TOKENS, MODEL_WIDTH), 1.0, 6.0, ((0, 4), (1, 4)))
    decay_input_part = draw_decay_input_part(jax.random.fold_in(jax.random.fold_in(streams_of[19], part), 71), part)
    correction_rate_input = draw_correction_rate_input(jax.random.fold_in(jax.random.fold_in(streams_of[19], part), 71), part)
    head_decay_offset = draw_head_decay_offset(jax.random.fold_in(jax.random.fold_in(streams_of[19], part), 71), part)
    decay_fixed_bias = draw_decay_fixed_bias(jax.random.fold_in(streams_of[19], 71), part)
    correction_rate_bias = draw_correction_rate_bias(jax.random.fold_in(streams_of[19], 71), part)
    head_norm_gain = jnp.clip(1.0 + 0.18 * jax.random.normal(streams_of[9], (MODEL_WIDTH,), jnp.float32), 0.1, 1.9)
    self_term_weight = bell_draw(streams_of[10], (MODEL_WIDTH,), 0.15, 2.0, ((0, 4),), jnp.float32)
    output_weight_matrix = bell_draw(streams_of[11], (MODEL_WIDTH, D), MODEL_WIDTH ** -0.5, 0.125, ((0, 4),))
    residual = bell_draw(own_keys[12], (SEQUENCE_TOKENS, D), 1.0, 6.0, ((0, 16),))
    feedforward_norm_gain = jnp.clip(1.0 + 0.18 * jax.random.normal(streams_of[13], (D,), jnp.float32), 0.1, 1.9)
    routed_expert_index_keys = jax.random.split(jax.random.fold_in(own_keys[14], 1), SEQUENCE_TOKENS // (TOK_SP // N_TP))
    routed_expert_index_turns = jax.random.permutation(jax.random.fold_in(own_keys[14], 3), SEQUENCE_TOKENS // (TOK_SP // N_TP))
    routed_expert_index = jax.vmap(lambda own, number: routed_block(jax.random.fold_in(own_keys[14], 2), own, number, TOK_SP // N_TP, EXPERTS, 2, CAP, 1))(routed_expert_index_keys, routed_expert_index_turns).reshape((SEQUENCE_TOKENS, 2))
    routed_expert_weight = jnp.clip(0.2 + 0.8 * jax.random.uniform(own_keys[15], (SEQUENCE_TOKENS, 2), jnp.float32) ** level_of(own_keys[15], (SEQUENCE_TOKENS, 2), ((0, 16),), -0.2, 0.2), 0.2, 1.0)
    gate_weight_experts = bell_draw(streams_of[16], (EXPERTS, D, FF), D ** -0.5, 0.125, ((0, 4), (2, 4)))
    up_weight_experts = bell_draw(streams_of[17], (EXPERTS, D, FF), D ** -0.5, 0.125, ((0, 4), (2, 4)))
    down_weight_experts = bell_draw(streams_of[18], (EXPERTS, FF, D), FF ** -0.5, 0.1875, ((0, 4), (1, 4)))
    return {"recept": recept, "key_input": key_input, "value_input": value_input, "output_gate_input": output_gate_input, "decay_input_part": decay_input_part, "correction_rate_input": correction_rate_input, "head_decay_offset": head_decay_offset, "decay_fixed_bias": decay_fixed_bias, "correction_rate_bias": correction_rate_bias, "head_norm_gain": head_norm_gain, "self_term_weight": self_term_weight, "output_weight_matrix": output_weight_matrix, "residual": residual, "feedforward_norm_gain": feedforward_norm_gain, "routed_expert_index": routed_expert_index, "routed_expert_weight": routed_expert_weight, "gate_weight_experts": gate_weight_experts, "up_weight_experts": up_weight_experts, "down_weight_experts": down_weight_experts}


PRECISE = lax.Precision.HIGHEST
GROUP_EPS = 0.00064
NORM_EPS = 1e-06

def recurrence(receptance_per_head, decay_per_head, key_per_head, value_per_head, remove_h, write_h):

    def advance(states, inputs):
        recept_t, decay_t, key_t, value_t, remove_t, write_t = inputs
        removed = jnp.einsum('hvk,hk->hv', states, remove_t, precision=PRECISE)
        states = states * decay_t[:, None, :] + removed[:, :, None] * write_t[:, None, :] + value_t[:, :, None] * key_t[:, None, :]
        return (states, jnp.einsum('hvk,hk->hv', states, recept_t, precision=PRECISE))
    initial = jnp.zeros((HEAD_COUNT, HEAD_CHANNELS, HEAD_CHANNELS), jnp.float32)
    _, readout = lax.scan(advance, initial, (receptance_per_head, decay_per_head, key_per_head, value_per_head, remove_h, write_h))
    return readout

def expert_rows(features, gate_mat, up_mat, down_mat):
    gated = jnp.dot(features, gate_mat, preferred_element_type=jnp.float32)
    upward = jnp.dot(features, up_mat, preferred_element_type=jnp.float32)
    hidden = (jax.nn.silu(gated) * upward).astype(jnp.bfloat16)
    blocks = jnp.einsum('rjf,jfd->rjd', hidden.reshape(features.shape[0], N_TP, FF // N_TP).astype(jnp.float32), down_mat.reshape(N_TP, FF // N_TP, D).astype(jnp.float32), precision=PRECISE)
    rounded = lax.optimization_barrier(blocks.astype(jnp.bfloat16)).astype(jnp.float32)
    return lax.optimization_barrier(jnp.sum(rounded, axis=1)).astype(jnp.bfloat16)

def reference(recept, key_input, value_input, output_gate_input, decay_input_part, correction_rate_input, head_decay_offset, decay_fixed_bias, correction_rate_bias, head_norm_gain, self_term_weight, output_weight_matrix, residual, feedforward_norm_gain, routed_expert_index, routed_expert_weight, gate_weight_experts, up_weight_experts, down_weight_experts):

    def split_into_heads(tensor):
        return tensor.astype(jnp.float32).reshape(SEQUENCE_TOKENS, HEAD_COUNT, HEAD_CHANNELS)
    receptance_per_head, key_per_head, value_per_head = (split_into_heads(recept), split_into_heads(key_input), split_into_heads(value_input))
    weight_logarithm = -jax.nn.softplus(-(decay_fixed_bias + decay_input_part.astype(jnp.float32))) - 0.5
    decay_per_head = jnp.exp(-jnp.exp(split_into_heads(weight_logarithm)) + head_decay_offset[:, :, None])
    rate_h = split_into_heads(jax.nn.sigmoid(correction_rate_bias + correction_rate_input.astype(jnp.float32)))
    unit_key = key_per_head * lax.rsqrt(lax.optimization_barrier(jnp.sum(key_per_head * key_per_head, axis=-1, keepdims=True)) + NORM_EPS)
    readout = recurrence(receptance_per_head, decay_per_head, key_per_head, value_per_head, -unit_key, unit_key * rate_h)
    center = lax.optimization_barrier(jnp.mean(readout, axis=-1, keepdims=True))
    spread = lax.optimization_barrier(jnp.mean(jnp.square(readout - center), axis=-1, keepdims=True))
    normalized_state = (readout - center) * lax.rsqrt(spread + GROUP_EPS) * head_norm_gain.reshape(HEAD_COUNT, HEAD_CHANNELS)
    self_term = lax.optimization_barrier(jnp.sum(receptance_per_head * key_per_head * self_term_weight.reshape(HEAD_COUNT, HEAD_CHANNELS), axis=-1, keepdims=True)) * value_per_head
    attention_result = ((normalized_state + self_term).reshape(SEQUENCE_TOKENS, MODEL_WIDTH) * output_gate_input.astype(jnp.float32)).astype(jnp.bfloat16)
    proj = jnp.dot(attention_result, output_weight_matrix, preferred_element_type=jnp.float32).astype(jnp.bfloat16)
    stream = residual.astype(jnp.float32) + lax.optimization_barrier(proj).astype(jnp.float32)
    ffn_in = (stream * lax.rsqrt(lax.optimization_barrier(jnp.mean(stream * stream, axis=-1, keepdims=True)) + NORM_EPS) * feedforward_norm_gain).astype(jnp.bfloat16)
    flat_ids = routed_expert_index.reshape(-1).astype(jnp.int32)
    flat_weights = routed_expert_weight.reshape(-1)
    top_count = routed_expert_index.shape[1]
    order = jnp.argsort(flat_ids, stable=True).astype(jnp.int32)
    counts = lax.optimization_barrier(jnp.sum((flat_ids[:, None] == jnp.arange(EXPERTS, dtype=jnp.int32)[None, :]).astype(jnp.int32), axis=0))
    starts = (jnp.cumsum(counts) - counts).astype(jnp.int32)
    room = N_SP * N_TP * CAP
    padded = jnp.concatenate([order, jnp.zeros((room,), jnp.int32)])

    def one_expert(accum, expert):
        entries = lax.dynamic_slice_in_dim(padded, starts[expert], room)
        live = jnp.arange(room, dtype=jnp.int32) < counts[expert]
        positions = (entries // top_count).astype(jnp.int32)
        result = expert_rows(ffn_in[positions], gate_weight_experts[expert], up_weight_experts[expert], down_weight_experts[expert])
        scales = jnp.where(live, flat_weights[entries], 0.0)
        return (accum.at[positions].add(result.astype(jnp.float32) * scales[:, None]), None)
    accum, _ = lax.scan(one_expert, jnp.zeros((SEQUENCE_TOKENS, D), jnp.float32), jnp.arange(EXPERTS, dtype=jnp.int32))
    return (stream + accum).astype(jnp.bfloat16)
```

```python
import functools

import jax
import jax.numpy as jnp
from jax import lax
from jax.experimental import pallas as pl
from jax.experimental.pallas import tpu as pltpu
from jax.sharding import PartitionSpec as P

SPAN = 64
SUB = 16
LANES = 256
GROUP_EPS = 0.00064
NORM_EPS = 1e-06
NN = (((1,), (0,)), ((), ()))
NT = (((1,), (1,)), ((), ()))
MESH = pl.DeviceIdType.MESH
VMEM_LIMIT = 60 * 1024 * 1024


def peer(**coords):
    return tuple(coords.get(name, lax.axis_index(name)) for name in ("grp", "sp", "tp"))


def tp_peers():
    place = lax.axis_index("tp")
    chip, core = place // 2, place % 2
    return 2 * chip + 1 - core, 2 * (1 - chip) + core, 2 * (1 - chip) + 1 - core


def remote(src, dst, send_sem, recv_sem, device):
    return pltpu.make_async_remote_copy(
        src_ref=src,
        dst_ref=dst,
        send_sem=send_sem,
        recv_sem=recv_sem,
        device_id=device,
        device_id_type=MESH,
    )


def greet(barrier, device):
    pl.semaphore_signal(barrier, inc=1, device_id=device, device_id_type=MESH)


def halves(x):
    high = x.astype(jnp.bfloat16)
    return high, (x - high.astype(jnp.float32)).astype(jnp.bfloat16)


def product(left, right, dims):
    def dot(a, b):
        return lax.dot_general(a, b, dims, preferred_element_type=jnp.float32)

    return dot(left[0], right[0]) + (dot(left[1], right[0]) + dot(left[0], right[1]))


def block_mask(head_width):
    rows = lax.broadcasted_iota(jnp.int32, (LANES, LANES), 0) // head_width
    lanes = lax.broadcasted_iota(jnp.int32, (LANES, LANES), 1) // head_width
    return jnp.where(rows == lanes, 1.0, 0.0)


def spread_blocks(x, mask):
    copies = LANES // x.shape[0]
    return tuple(jnp.concatenate([part] * copies, axis=0) * mask for part in halves(x))


def head_sum(x, mask):
    high, low = halves(x)
    return lax.dot_general(
        high, mask, NN, preferred_element_type=jnp.float32
    ) + lax.dot_general(low, mask, NN, preferred_element_type=jnp.float32)


class Gather:
    def __init__(self, own, full, sems):
        self.own, self.full = own, full
        (
            self.core_send,
            self.core_recv,
            self.chip_send,
            self.chip_recv,
            self.swap_send,
            self.swap_recv,
            self.pass_send,
            self.pass_recv,
        ) = sems
        near, far, _ = tp_peers()
        self.group = lax.axis_index("grp")
        self.near, self.far = peer(tp=near), peer(tp=far)
        self.twin = peer(grp=1 - self.group)

    def enter(self, others):
        barrier = pltpu.get_barrier_semaphore()
        for device in (self.near, self.far, self.twin):
            greet(barrier, device)
        pl.semaphore_wait(barrier, 3 + others(barrier))

    def half(self, ref, which):
        rows = ref.shape[0] // 2
        return ref.at[pl.ds(pl.multiple_of(which * rows, rows), rows)]

    def core_copy(self, k):
        return remote(
            self.own[k], self.full[k].at[0], self.core_send.at[k], self.core_recv.at[k], self.near
        )

    def chip_copy(self, k):
        return remote(
            self.half(self.own[k], self.group),
            self.half(self.full[k].at[1], self.group),
            self.chip_send.at[k],
            self.chip_recv.at[k],
            self.far,
        )

    def swap_copy(self, k):
        piece = self.half(self.full[k].at[1], self.group)
        return remote(piece, piece, self.swap_send.at[k], self.swap_recv.at[k], self.twin)

    def pass_copy(self, k, swapped):
        which = 1 - self.group if swapped else self.group
        slot = 2 * k + swapped
        return remote(
            self.half(self.full[k].at[1], which),
            self.half(self.full[k].at[2], which),
            self.pass_send.at[slot],
            self.pass_recv.at[slot],
            self.near,
        )

    def begin(self):
        for k in range(3):
            self.chip_copy(k).start()
        for k in range(3):
            self.core_copy(k).start()

    def arrive_chip(self, k):
        self.chip_copy(k).wait_recv()
        self.swap_copy(k).start()
        self.pass_copy(k, 0).start()

    def arrive_swap(self, k):
        piece = self.half(self.full[k].at[1], 1 - self.group)
        remote(piece, piece, self.swap_send.at[k], self.swap_recv.at[k], self.twin).wait_recv()
        self.pass_copy(k, 1).start()

    def middle(self, k):
        self.arrive_chip(k)
        if k > 0:
            self.arrive_swap(k - 1)

    def end(self):
        self.arrive_swap(2)
        for k in range(3):
            self.core_copy(k).wait()
            self.chip_copy(k).wait_send()
            self.swap_copy(k).wait_send()
            for swapped in range(2):
                self.pass_copy(k, swapped).wait()


class Spread:
    def __init__(self, own, full, send, recv, local):
        self.own, self.full, self.send, self.recv, self.local = own, full, send, recv, local
        self.count = lax.axis_size("sp")
        self.place = lax.axis_index("sp")

    def greet(self, barrier):
        def one(ahead, carry):
            greet(barrier, peer(sp=(self.place + ahead) % self.count))
            return carry

        lax.fori_loop(1, self.count, one, 0)
        return self.count - 1

    def copy(self, ahead):
        return remote(
            self.own,
            self.full.at[self.place],
            self.send.at[ahead - 1],
            self.recv.at[self.place],
            peer(sp=(self.place + ahead) % self.count),
        )

    def arrival(self, ahead):
        source = (self.place + self.count - ahead) % self.count
        return remote(
            self.own,
            self.full.at[source],
            self.send.at[ahead - 1],
            self.recv.at[source],
            peer(sp=source),
        )

    def begin(self):
        pltpu.make_async_copy(self.own, self.full.at[self.place], self.local).start()

        def one(ahead, carry):
            self.copy(ahead).start()
            return carry

        lax.fori_loop(1, self.count, one, 0)

    def end(self):
        pltpu.make_async_copy(self.own, self.full.at[self.place], self.local).wait()

        def one(ahead, carry):
            self.copy(ahead).wait_send()
            self.arrival(ahead).wait_recv()
            return carry

        lax.fori_loop(1, self.count, one, 0)


def chunk_kernel(
    head_width,
    recept_ref,
    key_ref,
    value_ref,
    decay_ref,
    rate_ref,
    offset_ref,
    decay_bias_ref,
    rate_bias_ref,
    share_ref,
    gate_ref,
    up_ref,
    down_ref,
    map_ref,
    own_ref,
    transit_ref,
    added_ref,
    shares_ref,
    gates_ref,
    ups_ref,
    downs_ref,
    core_send,
    core_recv,
    chip_send,
    chip_recv,
    swap_send,
    swap_recv,
    pass_send,
    pass_recv,
    share_send,
    share_recv,
    local_sem,
):
    weights = Gather(
        (gate_ref, up_ref, down_ref),
        (gates_ref, ups_ref, downs_ref),
        (core_send, core_recv, chip_send, chip_recv, swap_send, swap_recv, pass_send, pass_recv),
    )
    shares = Spread(share_ref, shares_ref, share_send, share_recv, local_sem)
    step = pl.program_id(0)
    last_step = pl.num_programs(0) - 1

    @pl.when(step == 0)
    def _():
        weights.enter(shares.greet)
        weights.begin()
        shares.begin()

    for number in range(1, 4):
        pl.when(step == number)(functools.partial(weights.middle, number - 1))

    span = head_width
    wide_mask = block_mask(head_width)
    mask = wide_mask.astype(jnp.bfloat16)
    per_group = LANES // head_width
    times = lax.broadcasted_iota(jnp.int32, (span, LANES), 0)
    lanes = lax.broadcasted_iota(jnp.int32, (span, LANES), 1)
    earlier = lanes % head_width
    strict = times > earlier
    within = times >= earlier
    eye = jnp.where(times == earlier, 1.0, 0.0)
    same = (times // SUB) == (earlier // SUB)
    tri = jnp.where(
        lax.broadcasted_iota(jnp.int32, (span, span), 0)
        >= lax.broadcasted_iota(jnp.int32, (span, span), 1),
        1.0,
        0.0,
    ).astype(jnp.bfloat16)

    @pl.when(pl.program_id(0) == 0)
    def _():
        full_lanes = lax.broadcasted_iota(jnp.int32, transit_ref.shape, 1) % head_width
        full_rows = lax.broadcasted_iota(jnp.int32, transit_ref.shape, 0)
        transit_ref[...] = jnp.where(full_lanes == full_rows, 1.0, 0.0)
        added_ref[...] = jnp.zeros_like(added_ref)

    spread = functools.partial(spread_blocks, mask=mask)
    row_count, channel_width = recept_ref.shape
    cells = [
        (group, chunk)
        for chunk in range(row_count // span)
        for group in range(channel_width // LANES)
    ]

    def prepare(group, chunk):
        at = (slice(chunk * span, (chunk + 1) * span), slice(group * LANES, (group + 1) * LANES))
        cols = at[1]
        recept = recept_ref[at].astype(jnp.float32)
        key = key_ref[at].astype(jnp.float32)
        value = value_ref[at].astype(jnp.float32)
        offset = jnp.zeros((span, LANES), jnp.float32)
        for head in range(per_group):
            column = group * per_group + head
            offset = jnp.where(
                lanes // head_width == head, offset_ref[at[0], column : column + 1], offset
            )
        pre = decay_bias_ref[:, cols] + decay_ref[at].astype(jnp.float32)
        decay = offset - 0.6065306597126334 / (1.0 + jnp.exp(-pre))
        rate = 1.0 / (
            1.0 + jnp.exp(-(rate_bias_ref[:, cols] + rate_ref[at].astype(jnp.float32)))
        )
        unit = key * lax.rsqrt(head_sum(key * key, mask) + NORM_EPS)
        one, rest = halves(decay)
        third = (decay - one.astype(jnp.float32) - rest.astype(jnp.float32)).astype(jnp.bfloat16)
        cumul = sum(
            lax.dot_general(tri, part, NN, preferred_element_type=jnp.float32)
            for part in (third, rest, one)
        )
        middle = cumul[span // 2 : span // 2 + 1]
        last = cumul[span - 1 : span]
        center = cumul - middle
        shrink = jnp.exp(center)
        grow = jnp.exp(-center)
        remove = -unit * jnp.exp(center - decay)
        reads = recept * shrink
        write = unit * rate * grow
        keys = key * grow
        left = halves(jnp.concatenate([remove, reads], axis=0))
        by_write = product(left, spread(write), NT)
        by_key = product(left, spread(keys), NT)
        remove_write = jnp.where(strict, by_write[:span], 0.0)
        read_write = halves(jnp.where(within, by_write[span:], 0.0))
        key_rows = halves(
            jnp.concatenate(
                [jnp.where(strict, by_key[:span], 0.0), jnp.where(within, by_key[span:], 0.0)],
                axis=0,
            )
        )
        power = jnp.where(same, remove_write, 0.0)
        inverse = eye + power
        power = product(halves(power), spread(power), NN)
        reach = 2
        while reach < SUB:
            factor = spread(power)
            if reach * 2 < SUB:
                both = product(
                    halves(jnp.concatenate([inverse, power], axis=0)), factor, NN
                )
                inverse = inverse + both[:span]
                power = both[span:]
            else:
                inverse = inverse + product(halves(inverse), factor, NN)
            reach *= 2
        size = SUB
        while size < span:
            joint = (times // (2 * size) == earlier // (2 * size)) & (
                times // size != earlier // size
            )
            step = product(
                halves(inverse), spread(jnp.where(joint, remove_write, 0.0)), NN
            )
            inverse = inverse + product(halves(step), spread(inverse), NN)
            size *= 2
        inverse = halves(inverse)
        start = jnp.exp(middle)
        from_value = product(key_rows, spread(value), NN)
        inv_remove = product(inverse, spread(remove), NN) * start
        inv_value = product(inverse, spread(from_value[:span]), NN)
        read_map = reads * start + product(read_write, spread(inv_remove), NN)
        read_own = from_value[span:] + product(read_write, spread(inv_value), NN)
        tail = jnp.exp(last - middle)
        write_end = write * tail
        key_end = keys * tail
        transit = product(halves(inv_remove.T), halves(write_end), NN)
        transit = transit * wide_mask
        full = jnp.concatenate([jnp.exp(last)] * (LANES // 8), axis=0)
        full = jnp.concatenate([full] * 8, axis=0)
        diagonal = lax.broadcasted_iota(jnp.int32, (LANES, LANES), 0) == (
            lax.broadcasted_iota(jnp.int32, (LANES, LANES), 1)
        )
        transit = transit + jnp.where(diagonal, full, 0.0)
        added = product(
            halves(jnp.concatenate([inv_value, value], axis=0).T),
            halves(jnp.concatenate([write_end, key_end], axis=0)),
            NN,
        )
        added = added * wide_mask
        added = sum(added[h * head_width : (h + 1) * head_width] for h in range(per_group))
        return at, read_map, read_own, transit, added

    for group, chunk in cells:
        at, read_map, read_own, transit, added = prepare(group, chunk)
        cols = at[1]
        held_transit = transit_ref[:, cols]
        held_added = added_ref[:, cols]
        rows = halves(read_map)
        map_ref[at] = product(rows, spread(held_transit), NT)
        own_ref[at] = read_own + product(rows, spread(held_added), NT)
        moved = product(
            halves(jnp.concatenate([held_transit, held_added], axis=0)), halves(transit), NN
        )
        transit_ref[:, cols] = moved[:span]
        added_ref[:, cols] = moved[span:] + added

    @pl.when(step == last_step)
    def _():
        weights.end()
        shares.end()


def mixed_rows(head_width, rows, state, refs, mask):
    map_ref, own_ref, recept_ref, key_ref, value_ref, gate_ref, gain_ref, self_ref = refs
    parts = []
    for group in range(map_ref.shape[1] // LANES):
        cols = slice(group * LANES, (group + 1) * LANES)
        read = own_ref[rows, cols] + product(
            halves(map_ref[rows, cols]), spread_blocks(state[group], mask), NT
        )
        off = read - head_sum(read, mask) * (1.0 / head_width)
        spread = head_sum(off * off, mask) * (1.0 / head_width)
        normed = off * lax.rsqrt(spread + GROUP_EPS) * gain_ref[:, cols]
        value = value_ref[rows, cols].astype(jnp.float32)
        own = (
            head_sum(
                recept_ref[rows, cols].astype(jnp.float32)
                * key_ref[rows, cols].astype(jnp.float32)
                * self_ref[:, cols],
                mask,
            )
            * value
        )
        parts.append(
            ((normed + own) * gate_ref[rows, cols].astype(jnp.float32)).astype(jnp.bfloat16)
        )
    return parts


def middle_kernel(
    head_width,
    map_ref,
    own_ref,
    transit_ref,
    added_ref,
    recept_ref,
    key_ref,
    value_ref,
    gate_ref,
    gain_ref,
    self_ref,
    out_weight_ref,
    residual_ref,
    norm_gain_ref,
    stream_ref,
    features_ref,
    state_ref,
    onward_ref,
    core_out,
    core_in,
    chip_out,
    chip_in,
    state_send,
    state_recv,
    core_send,
    core_recv,
    chip_send,
    chip_recv,
):
    place, count = lax.axis_index("sp"), lax.axis_size("sp")
    near, far, cross = tp_peers()
    mine = lax.axis_index("tp")
    groups = map_ref.shape[1] // LANES
    rows = residual_ref.shape[0]
    parts = chip_out.shape[0]
    mask = block_mask(head_width).astype(jnp.bfloat16)
    barrier = pltpu.get_barrier_semaphore()
    greet(barrier, peer(tp=near))
    greet(barrier, peer(tp=far))
    ahead, behind = peer(sp=(place + 1) % count), peer(sp=(place + count - 1) % count)

    @pl.when(place > 0)
    def _():
        greet(barrier, behind)

    @pl.when(place < count - 1)
    def _():
        greet(barrier, ahead)

    pl.semaphore_wait(
        barrier, 2 + jnp.where(place > 0, 1, 0) + jnp.where(place < count - 1, 1, 0)
    )

    def state_copy(group):
        return remote(
            onward_ref.at[group],
            state_ref.at[group],
            state_send.at[group],
            state_recv.at[group],
            ahead,
        )

    @pl.when(place == 0)
    def _():
        for group in range(groups):
            cols = slice(group * LANES, (group + 1) * LANES)
            state_ref[group] = jnp.zeros_like(state_ref[group])
            onward_ref[group] = added_ref[:, cols]
            state_copy(group).start()

    @pl.when(place > 0)
    def _():
        for group in range(groups):
            cols = slice(group * LANES, (group + 1) * LANES)
            state_copy(group).wait_recv()

            @pl.when(place < count - 1)
            def _(group=group, cols=cols):
                onward_ref[group] = added_ref[:, cols] + product(
                    halves(state_ref[group]), spread_blocks(transit_ref[:, cols], mask), NN
                )
                state_copy(group).start()

    refs = (map_ref, own_ref, recept_ref, key_ref, value_ref, gate_ref, gain_ref, self_ref)

    def partial(owner, part):
        size = rows // parts
        at = pl.ds(pl.multiple_of(owner * rows + part * size, size), size)
        total = None
        for group, mixed in enumerate(
            mixed_rows(head_width, at, [state_ref[g] for g in range(groups)], refs, mask)
        ):
            term = lax.dot_general(
                mixed,
                out_weight_ref[group * LANES : (group + 1) * LANES],
                NN,
                preferred_element_type=jnp.float32,
            )
            total = term if total is None else total + term
        return total

    def core_copy(which, part):
        slot = which * parts + part
        return remote(
            core_out.at[slot],
            core_in.at[slot],
            core_send.at[slot],
            core_recv.at[slot],
            peer(tp=near),
        )

    def chip_copy(part):
        return remote(
            chip_out.at[part],
            chip_in.at[part],
            chip_send.at[part],
            chip_recv.at[part],
            peer(tp=far),
        )

    for part in range(parts):
        core_out[part] = partial(cross, part)
        core_copy(0, part).start()
        own = partial(far, part)
        core_copy(0, part).wait_recv()
        chip_out[part] = (own + core_in[part]).astype(jnp.bfloat16)
        chip_copy(part).start()
    for part in range(parts):
        core_out[parts + part] = partial(near, part)
        core_copy(1, part).start()
        own = partial(mine, part)
        core_copy(1, part).wait_recv()
        size = rows // parts
        stream_ref[part * size : (part + 1) * size] = (
            residual_ref[part * size : (part + 1) * size].astype(jnp.float32)
            + own
            + core_in[parts + part]
        )
    for part in range(parts):
        size = rows // parts
        at = slice(part * size, (part + 1) * size)
        chip_copy(part).wait_recv()
        stream = stream_ref[at] + chip_in[part].astype(jnp.float32)
        stream_ref[at] = stream
        features_ref[at] = (
            stream
            * lax.rsqrt(jnp.mean(stream * stream, axis=-1, keepdims=True) + NORM_EPS)
            * norm_gain_ref[...]
        ).astype(jnp.bfloat16)

    @pl.when(place < count - 1)
    def _():
        for group in range(groups):
            state_copy(group).wait_send()

    for part in range(parts):
        core_copy(0, part).wait_send()
        core_copy(1, part).wait_send()
        chip_copy(part).wait_send()


def expert_kernel(
    pieces,
    lag,
    features_ref,
    stream_ref,
    shares_ref,
    gate_ref,
    up_ref,
    down_ref,
    gates_ref,
    ups_ref,
    downs_ref,
    out_ref,
    gate_all,
    up_all,
    down_all,
    blocks,
    result,
    from_right,
    from_left,
    to_left,
    to_right,
    load_sem,
    gather_send,
    gather_recv,
    sum_send,
    sum_recv,
):
    place, count = lax.axis_index("sp"), lax.axis_size("sp")
    left, right = peer(sp=(place + count - 1) % count), peer(sp=(place + 1) % count)
    has_left, has_right = place > 0, place < count - 1
    size = features_ref.shape[0] // pieces
    loads = []
    for k, (own, rest, full) in enumerate(
        ((gate_ref, gates_ref, gate_all), (up_ref, ups_ref, up_all), (down_ref, downs_ref, down_all))
    ):
        loads.append(pltpu.make_async_copy(own, full.at[0], load_sem.at[2 * k]))
        loads.append(
            pltpu.make_async_copy(rest, full.at[pl.ds(1, rest.shape[0])], load_sem.at[2 * k + 1])
        )
    for load in loads:
        load.start()
    barrier = pltpu.get_barrier_semaphore()
    for there, device in ((has_left, left), (has_right, right)):
        pl.when(there)(functools.partial(greet, barrier, device))
    pl.semaphore_wait(barrier, jnp.where(has_left, 1, 0) + jnp.where(has_right, 1, 0))

    def gather_copy(source, block, piece, way):
        return remote(
            source,
            blocks.at[block, piece],
            gather_send.at[way, block, piece],
            gather_recv.at[block, piece],
            right if way else left,
        )

    def sum_copy(block, piece, way):
        out, into = (to_right, from_left) if way else (to_left, from_right)
        return remote(
            out.at[block, piece],
            into.at[block, piece],
            sum_send.at[way, block, piece],
            sum_recv.at[way, block, piece],
            right if way else left,
        )

    for piece in range(pieces):
        mine = features_ref.at[pl.ds(piece * size, size)]
        for way, there in ((0, has_left), (1, has_right)):
            pl.when(there)(lambda: gather_copy(mine, place, piece, way).start())

    def apply(features, block, piece):
        total = None
        for j in range(gate_all.shape[0]):
            gated = lax.dot_general(
                features, gate_all[j], NN, preferred_element_type=jnp.float32
            )
            upward = lax.dot_general(features, up_all[j], NN, preferred_element_type=jnp.float32)
            hidden = (jax.nn.silu(gated) * upward).astype(jnp.bfloat16)
            term = lax.dot_general(hidden, down_all[j], NN, preferred_element_type=jnp.float32)
            total = term if total is None else total + term
        weights = shares_ref[block, pl.ds(pl.multiple_of(piece * size, size), size)]
        lanes = lax.broadcasted_iota(jnp.int32, weights.shape, 1)
        share = jnp.sum(jnp.where(lanes == place, weights, 0.0), axis=1, keepdims=True)
        result[block, piece] = total * share

    for load in loads:
        load.wait()

    def own_piece(piece, carry):
        apply(
            features_ref[pl.ds(pl.multiple_of(piece * size, size), size)], place, piece
        )
        return carry

    lax.fori_loop(0, pieces, own_piece, 0)

    def slot(time, carry):
        distance, piece = time // pieces + 1, time % pieces
        for way, block, there, onward in (
            (1, place - distance, place - distance >= 0, has_right),
            (0, place + distance, place + distance < count, has_left),
        ):

            @pl.when(there)
            def _(way=way, block=block, onward=onward):
                landed = blocks.at[block, piece]
                gather_copy(landed, block, piece, way).wait_recv()
                pl.when(onward)(lambda: gather_copy(landed, block, piece, way).start())

        for block, there in (
            (place - distance, place - distance >= 0),
            (place + distance, place + distance < count),
        ):

            @pl.when(there)
            def _(block=block):
                apply(blocks[block, piece], block, piece)

        for way, hops, first, step, more, into, out in (
            (0, count - 1 - place, count - 2, -1, has_right, from_right, to_left),
            (1, place, 1, 1, has_left, from_left, to_right),
        ):
            turn = time - lag * hops
            block = first + step * (turn // pieces)
            part = turn % pieces
            passed = (place - block) * (1 - 2 * way)
            valid = (turn >= 0) & (block >= 0) & (block < count) & (passed >= 0)

            @pl.when(valid & more)
            def _(way=way, block=block, part=part, into=into):
                sum_copy(block, part, way).wait_recv()
                result[block, part] = result[block, part] + into[block, part].astype(jnp.float32)

            @pl.when(valid & (passed > 0))
            def _(way=way, block=block, part=part, out=out):
                out[block, part] = result[block, part].astype(jnp.bfloat16)
                sum_copy(block, part, way).start()

        return carry

    lax.fori_loop(0, (count - 1) * pieces + lag * (count - 1), slot, 0)
    for piece in range(pieces):
        at = slice(piece * size, (piece + 1) * size)
        out_ref[at] = (stream_ref[at] + result[place, piece]).astype(out_ref.dtype)

    def drain(block, carry):
        for piece in range(pieces):
            landed = blocks.at[block, piece]
            for way, gathers, sums in (
                (0, has_left & (block >= place), has_left & (block < place)),
                (1, has_right & (block <= place), has_right & (block > place)),
            ):
                pl.when(gathers)(
                    lambda: gather_copy(landed, block, piece, way).wait_send()
                )
                pl.when(sums)(lambda: sum_copy(block, piece, way).wait_send())
        return carry

    lax.fori_loop(0, count, drain, 0)


def shares_of(routed_expert_index, routed_expert_weight, experts):
    ids = jnp.arange(experts, dtype=jnp.int32)
    shares = jnp.sum(
        jnp.where(
            routed_expert_index[:, :, None] == ids, routed_expert_weight[:, :, None], 0.0
        ),
        axis=1,
    )
    return jnp.pad(shares, ((0, 0), (0, -experts % 128)))


def experts_by_collectives(features, stream, shares, gates, ups, downs):
    features = lax.all_gather(features, "sp", axis=0, tiled=True)
    shares = shares.reshape(-1, shares.shape[-1])
    place = lax.axis_index("sp")
    lanes = jnp.arange(shares.shape[1], dtype=jnp.int32)
    share = jnp.sum(jnp.where(lanes[None, :] == place, shares, 0.0), axis=1, keepdims=True)
    depth = features.shape[1]

    def some_rows(operands):
        features, share = operands
        total = None
        for gate, up, down in zip(gates, ups, downs):
            for j in range(gate.shape[0]):
                gated = jnp.dot(features, gate[j], preferred_element_type=jnp.float32)
                upward = jnp.dot(features, up[j], preferred_element_type=jnp.float32)
                hidden = (jax.nn.silu(gated) * upward).astype(jnp.bfloat16)
                term = jnp.dot(hidden, down[j], preferred_element_type=jnp.float32)
                total = term if total is None else total + term
        return (total * share).astype(jnp.bfloat16)

    rows = stream.shape[0]
    total = lax.map(
        some_rows, (features.reshape(-1, rows, depth), share.reshape(-1, rows, 1))
    ).reshape(-1, depth)
    weighted = lax.psum_scatter(total, "sp", scatter_dimension=0, tiled=True)
    return (stream + weighted.astype(jnp.float32)).astype(jnp.bfloat16)


PIECES = 2
LAG = 2


def local(
    recept,
    key_input,
    value_input,
    output_gate_input,
    decay_input_part,
    correction_rate_input,
    head_decay_offset,
    decay_fixed_bias,
    correction_rate_bias,
    head_norm_gain,
    self_term_weight,
    output_weight_matrix,
    residual,
    feedforward_norm_gain,
    routed_expert_index,
    routed_expert_weight,
    gate_weight_experts,
    up_weight_experts,
    down_weight_experts,
):
    count = lax.axis_size("sp")
    experts = gate_weight_experts.shape[0] * count
    assert lax.axis_size("tp") == 4 and lax.axis_size("grp") == 2
    assert gate_weight_experts.shape[0] == 1
    length, width = recept.shape
    heads = head_decay_offset.shape[1]
    head_width = width // heads
    rows = 2 * SPAN
    own_rows, depth = residual.shape
    shares = shares_of(routed_expert_index, routed_expert_weight, experts)
    gate, up, down = gate_weight_experts[0], up_weight_experts[0], down_weight_experts[0]
    by_rows = pl.BlockSpec((rows, width), lambda i: (i, 0))
    fixed = pl.BlockSpec((1, width), lambda i: (0, 0))
    states = pl.BlockSpec((head_width, width), lambda i: (0, 0))
    anywhere = pl.BlockSpec(memory_space=pl.ANY)
    in_vmem = pl.BlockSpec(memory_space=pltpu.VMEM)
    wide = jax.ShapeDtypeStruct((length, width), jnp.float32)
    small = jax.ShapeDtypeStruct((head_width, width), jnp.float32)
    dma = pltpu.SemaphoreType.DMA

    def three(x):
        return jax.ShapeDtypeStruct((3, *x.shape), x.dtype)

    read_map, read_own, transit, added, all_shares, gates, ups, downs = pl.pallas_call(
        functools.partial(chunk_kernel, head_width),
        grid=(length // rows,),
        in_specs=[by_rows] * 5
        + [pl.BlockSpec((rows, heads), lambda i: (i, 0)), fixed, fixed]
        + [anywhere] * 4,
        out_specs=[by_rows, by_rows, states, states] + [anywhere] * 4,
        out_shape=[
            wide,
            wide,
            small,
            small,
            jax.ShapeDtypeStruct((count, *shares.shape), shares.dtype),
            three(gate),
            three(up),
            three(down),
        ],
        scratch_shapes=[dma((3,))] * 6
        + [dma((6,))] * 2
        + [dma((count,)), dma((count,)), dma],
        compiler_params=pltpu.CompilerParams(
            dimension_semantics=("arbitrary",),
            collective_id=0,
            has_side_effects=True,
            vmem_limit_bytes=32 * 1024 * 1024,
        ),
        cost_estimate=pl.CostEstimate(
            flops=30_000_000_000, bytes_accessed=8 * length * width, transcendentals=0
        ),
        name="chunks",
    )(
        recept,
        key_input,
        value_input,
        decay_input_part,
        correction_rate_input,
        head_decay_offset,
        decay_fixed_bias[None],
        correction_rate_bias[None],
        shares,
        gate,
        up,
        down,
    )
    groups = width // LANES
    half = own_rows // PIECES
    own_wide = jax.ShapeDtypeStruct((own_rows, depth), jnp.float32)
    own_narrow = jax.ShapeDtypeStruct((own_rows, depth), jnp.bfloat16)
    stream, features = pl.pallas_call(
        functools.partial(middle_kernel, head_width),
        in_specs=[in_vmem] * 13,
        out_specs=[in_vmem] * 2,
        out_shape=[own_wide, own_narrow],
        scratch_shapes=[
            pltpu.VMEM((groups, head_width, LANES), jnp.float32),
            pltpu.VMEM((groups, head_width, LANES), jnp.float32),
            pltpu.VMEM((2 * PIECES, half, depth), jnp.float32),
            pltpu.VMEM((2 * PIECES, half, depth), jnp.float32),
            pltpu.VMEM((PIECES, half, depth), jnp.bfloat16),
            pltpu.VMEM((PIECES, half, depth), jnp.bfloat16),
            dma((groups,)),
            dma((groups,)),
            dma((2 * PIECES,)),
            dma((2 * PIECES,)),
            dma((PIECES,)),
            dma((PIECES,)),
        ],
        compiler_params=pltpu.CompilerParams(
            collective_id=1, has_side_effects=True, vmem_limit_bytes=VMEM_LIMIT
        ),
        cost_estimate=pl.CostEstimate(
            flops=8_000_000_000, bytes_accessed=20 * length * width, transcendentals=0
        ),
        name="middle",
    )(
        read_map,
        read_own,
        transit,
        added,
        recept,
        key_input,
        value_input,
        output_gate_input,
        head_norm_gain[None],
        self_term_weight[None],
        output_weight_matrix,
        residual,
        feedforward_norm_gain[None],
    )
    if count > 4:
        return experts_by_collectives(
            features, stream, all_shares, (gate[None], gates), (up[None], ups), (down[None], downs)
        )
    flow = pltpu.VMEM((count, PIECES, half, depth), jnp.bfloat16)
    both = dma((2, count, PIECES))
    return pl.pallas_call(
        functools.partial(expert_kernel, PIECES, LAG),
        in_specs=[in_vmem] * 3 + [anywhere] * 6,
        out_specs=in_vmem,
        out_shape=own_narrow,
        scratch_shapes=[
            pltpu.VMEM((4, *gate.shape), gate.dtype),
            pltpu.VMEM((4, *up.shape), up.dtype),
            pltpu.VMEM((4, *down.shape), down.dtype),
            flow,
            pltpu.VMEM((count, PIECES, half, depth), jnp.float32),
            flow,
            flow,
            flow,
            flow,
            dma((6,)),
            both,
            dma((count, PIECES)),
            both,
            both,
        ],
        compiler_params=pltpu.CompilerParams(
            collective_id=2, has_side_effects=True, vmem_limit_bytes=VMEM_LIMIT
        ),
        cost_estimate=pl.CostEstimate(
            flops=8_000_000_000, bytes_accessed=20 * length * width, transcendentals=0
        ),
        name="experts",
    )(features, stream, all_shares, gate, up, down, gates, ups, downs)


def solution(mesh):
    return jax.shard_map(
        local,
        mesh=mesh,
        in_specs=(
            P(("grp", "sp"), "tp"),
            P(("grp", "sp"), "tp"),
            P(("grp", "sp"), "tp"),
            P(("grp", "sp"), "tp"),
            P(("grp", "sp"), "tp"),
            P(("grp", "sp"), "tp"),
            P(("grp", "sp"), "tp"),
            P("tp"),
            P("tp"),
            P("tp"),
            P("tp"),
            P("tp", None),
            P(("grp", "sp", "tp"), None),
            P(),
            P(("grp", "sp", "tp"), None),
            P(("grp", "sp", "tp"), None),
            P("sp", None, "tp"),
            P("sp", None, "tp"),
            P("sp", "tp", None),
        ),
        out_specs=P(("grp", "sp", "tp"), None),
        check_vma=False,
    )
```

```python
import functools
import types
import typing

import jax
import jax.numpy as jnp
from jax import lax
from jax.experimental import pallas as pl
from jax.experimental.pallas import tpu as pltpu
from jax.sharding import PartitionSpec as P

SPAN = 64
LANES = 256
GROUP_EPS = 0.00064
NORM_EPS = 1e-06
NN = (((1,), (0,)), ((), ()))
NT = (((1,), (1,)), ((), ()))
MESH = pl.DeviceIdType.MESH
VMEM_LIMIT = 60 * 1024 * 1024


def peer(**coords):
    return tuple(coords.get(name, lax.axis_index(name)) for name in ("grp", "sp", "tp"))


def tp_peers():
    place = lax.axis_index("tp")
    chip, core = place // 2, place % 2
    return 2 * chip + 1 - core, 2 * (1 - chip) + core, 2 * (1 - chip) + 1 - core


def remote(src, dst, send_sem, recv_sem, device):
    return pltpu.make_async_remote_copy(
        src_ref=src,
        dst_ref=dst,
        send_sem=send_sem,
        recv_sem=recv_sem,
        device_id=device,
        device_id_type=MESH,
    )


def greet(barrier, device):
    pl.semaphore_signal(barrier, inc=1, device_id=device, device_id_type=MESH)


def halves(x):
    high = x.astype(jnp.bfloat16)
    return high, (x - high.astype(jnp.float32)).astype(jnp.bfloat16)


def product(left, right, dims):
    def dot(a, b):
        return lax.dot_general(a, b, dims, preferred_element_type=jnp.float32)

    return dot(left[0], right[0]) + (dot(left[1], right[0]) + dot(left[0], right[1]))


def block_mask(head_width):
    rows = lax.broadcasted_iota(jnp.int32, (LANES, LANES), 0) // head_width
    lanes = lax.broadcasted_iota(jnp.int32, (LANES, LANES), 1) // head_width
    return jnp.where(rows == lanes, 1.0, 0.0)


def spread_blocks(x, mask):
    copies = LANES // x.shape[0]
    return tuple(jnp.concatenate([part] * copies, axis=0) * mask for part in halves(x))


def head_sum(x, mask):
    high, low = halves(x)
    return lax.dot_general(
        high, mask, NN, preferred_element_type=jnp.float32
    ) + lax.dot_general(low, mask, NN, preferred_element_type=jnp.float32)


PORTIONS = ((0, 0, 4), (0, 4, 4), (1, 0, 4), (1, 4, 4), (2, 0, 4), (2, 4, 2), (2, 6, 2))
LATE = len(PORTIONS) - 1


class Gather:
    def __init__(self, own, full, sems):
        self.own, self.full = own, full
        (
            self.core_send,
            self.core_recv,
            self.chip_send,
            self.chip_recv,
            self.swap_send,
            self.swap_recv,
            self.pass_send,
            self.pass_recv,
            self.load,
        ) = sems
        near, far, _ = tp_peers()
        self.group = lax.axis_index("grp")
        self.near, self.far = peer(tp=near), peer(tp=far)
        self.twin = peer(grp=1 - self.group)

    def portion(self, refs, index, which, slot=None):
        k, first, size = PORTIONS[index]
        ref = refs[k]
        rows = ref.shape[-2] // 2
        unit = rows // 8
        start = pl.multiple_of(which * rows + first * unit, unit)
        at = pl.ds(start, size * unit)
        return ref.at[at] if slot is None else ref.at[slot, at]

    def core_copy(self, k):
        return remote(
            self.own[k], self.full[k].at[1], self.core_send.at[k], self.core_recv.at[k], self.near
        )

    def chip_copy(self, index):
        return remote(
            self.portion(self.own, index, self.group),
            self.portion(self.full, index, self.group, 2),
            self.chip_send.at[index],
            self.chip_recv.at[index],
            self.far,
        )

    def swap_copy(self, index, which):
        piece = self.portion(self.full, index, which, 2)
        return remote(
            piece, piece, self.swap_send.at[index], self.swap_recv.at[index], self.twin
        )

    def pass_copy(self, index, swapped):
        which = 1 - self.group if swapped else self.group
        slot = 2 * index + swapped
        return remote(
            self.portion(self.full, index, which, 2),
            self.portion(self.full, index, which, 3),
            self.pass_send.at[slot],
            self.pass_recv.at[slot],
            self.near,
        )

    def load_copy(self, k):
        return pltpu.make_async_copy(self.own[k], self.full[k].at[0], self.load.at[k])

    def begin(self):
        for index in range(LATE):
            self.chip_copy(index).start()
        for k in range(3):
            self.core_copy(k).start()
            self.load_copy(k).start()

    def begin_late(self):
        self.chip_copy(LATE).start()

    def arrive_chip(self, index):
        self.chip_copy(index).wait_recv()
        self.swap_copy(index, self.group).start()
        self.pass_copy(index, 0).start()

    def arrive_swap(self, index):
        self.swap_copy(index, 1 - self.group).wait_recv()
        self.pass_copy(index, 1).start()

    def arrive_rest(self):
        self.arrive_swap(LATE)
        for k in range(3):
            self.load_copy(k).wait()
            self.core_copy(k).wait_recv()
        for index in range(len(PORTIONS)):
            for swapped in range(2):
                self.pass_copy(index, swapped).wait_recv()

    def drain(self):
        for k in range(3):
            self.core_copy(k).wait_send()
        for index in range(len(PORTIONS)):
            self.chip_copy(index).wait_send()
            self.swap_copy(index, self.group).wait_send()
            for swapped in range(2):
                self.pass_copy(index, swapped).wait_send()


class Spread:
    def __init__(self, own, full, send, recv):
        self.own, self.full, self.send, self.recv = own, full, send, recv
        self.count = lax.axis_size("sp")
        self.place = lax.axis_index("sp")

    def greet(self, barrier):
        def one(ahead, carry):
            greet(barrier, peer(sp=(self.place + ahead) % self.count))
            return carry

        lax.fori_loop(1, self.count, one, 0)
        return self.count - 1

    def copy(self, ahead):
        return remote(
            self.own,
            self.full.at[self.place],
            self.send.at[ahead - 1],
            self.recv.at[self.place],
            peer(sp=(self.place + ahead) % self.count),
        )

    def arrival(self, ahead):
        source = (self.place + self.count - ahead) % self.count
        return remote(
            self.own,
            self.full.at[source],
            self.send.at[ahead - 1],
            self.recv.at[source],
            peer(sp=source),
        )

    def begin(self):
        self.full[self.place] = self.own[...]

        def one(ahead, carry):
            self.copy(ahead).start()
            return carry

        lax.fori_loop(1, self.count, one, 0)

    def end(self):
        def one(ahead, carry):
            self.copy(ahead).wait_send()
            self.arrival(ahead).wait_recv()
            return carry

        lax.fori_loop(1, self.count, one, 0)


def single(left, right, dims=NN):
    return lax.dot_general(
        left.astype(jnp.bfloat16),
        right.astype(jnp.bfloat16),
        dims,
        preferred_element_type=jnp.float32,
    )


def chunk_cells(head_width, refs, cells, offsets):
    recept_ref, key_ref, value_ref, decay_ref, rate_ref, decay_bias, rate_bias = refs
    span = head_width
    per_group = LANES // head_width
    wide_mask = block_mask(head_width)
    mask = wide_mask.astype(jnp.bfloat16)
    times = lax.broadcasted_iota(jnp.int32, (span, LANES), 0)
    lanes = lax.broadcasted_iota(jnp.int32, (span, LANES), 1)
    earlier = lanes % head_width
    strict = times > earlier
    within = times >= earlier
    eye = jnp.where(times == earlier, 1.0, 0.0)
    tri_rows = lax.broadcasted_iota(jnp.int32, (span, 3 * span), 0)
    tri_lanes = lax.broadcasted_iota(jnp.int32, (span, 3 * span), 1) % span
    tri = jnp.where(tri_rows >= tri_lanes, 1.0, 0.0).astype(jnp.bfloat16)

    def spread(x):
        return jnp.concatenate([x.astype(jnp.bfloat16)] * per_group, axis=0) * mask

    def each(step, *lists):
        return [step(*values) for values in zip(*lists)]

    def load(ref):
        return [ref[rows, cols].astype(jnp.float32) for rows, cols in cells]

    recept, key, value = load(recept_ref), load(key_ref), load(value_ref)

    def decays(cell, extra, by_head):
        cols = cell[1]
        offset = jnp.zeros((span, LANES), jnp.float32)
        for head in range(per_group):
            column = cols.start // head_width + head
            offset = jnp.where(
                lanes // head_width == head, by_head[:, column : column + 1], offset
            )
        return offset - 0.6065306597126334 / (1.0 + jnp.exp(-(decay_bias[:, cols] + extra)))

    decay = each(decays, cells, load(decay_ref), offsets)
    rate = each(
        lambda cell, extra: 1.0 / (1.0 + jnp.exp(-(rate_bias[:, cell[1]] + extra))),
        cells,
        load(rate_ref),
    )
    norm = each(lambda k: single(k * k, mask), key)
    unit = each(lambda k, n: k * lax.rsqrt(n + NORM_EPS), key, norm)

    def cumulative(d):
        one, rest = halves(d)
        third = (d - one.astype(jnp.float32) - rest.astype(jnp.float32)).astype(jnp.bfloat16)
        return single(tri, jnp.concatenate([third, rest, one], axis=0))

    cumul = each(cumulative, decay)
    middle = [c[span // 2 : span // 2 + 1] for c in cumul]
    last = [c[span - 1 : span] for c in cumul]
    center = each(lambda c, m: c - m, cumul, middle)
    grow = each(lambda c: jnp.exp(-c), center)
    remove = each(lambda u, c, d: -u * jnp.exp(c - d), unit, center, decay)
    reads = each(lambda r, c: r * jnp.exp(c), recept, center)
    write = each(lambda u, r, g: u * r * g, unit, rate, grow)
    keys = each(lambda k, g: k * g, key, grow)
    left = each(
        lambda a, b: jnp.concatenate([a, b], axis=0).astype(jnp.bfloat16), remove, reads
    )
    by_write = each(lambda a, b: single(a, spread(b), NT), left, write)
    by_key = each(lambda a, b: single(a, spread(b), NT), left, keys)
    remove_write = [jnp.where(strict, x[:span], 0.0) for x in by_write]
    read_write = [jnp.where(within, x[span:], 0.0).astype(jnp.bfloat16) for x in by_write]
    key_rows = [
        jnp.concatenate(
            [jnp.where(strict, x[:span], 0.0), jnp.where(within, x[span:], 0.0)], axis=0
        )
        for x in by_key
    ]
    from_value = each(
        lambda a, b: sum(single(part, spread(b)) for part in halves(a)), key_rows, value
    )
    inverse = [eye + jnp.where(times // 2 == earlier // 2, x, 0.0) for x in remove_write]
    size = 2
    while size < span:
        joint = (times // (2 * size) == earlier // (2 * size)) & (
            times // size != earlier // size
        )
        step = each(
            lambda a, b: single(a, spread(jnp.where(joint, b, 0.0))), inverse, remove_write
        )
        inverse = each(lambda a, b: b + single(a, spread(b)), step, inverse)
        size *= 2
    start = [jnp.exp(m) for m in middle]
    inverse = [halves(x) for x in inverse]
    inv_remove = each(
        lambda a, b, c: product(a, spread_blocks(b, mask), NN) * c, inverse, remove, start
    )
    inv_value = each(
        lambda a, b: product(a, spread_blocks(b[:span], mask), NN), inverse, from_value
    )
    read_map = each(
        lambda a, b, c, d: a * b + single(c, spread(d)), reads, start, read_write, inv_remove
    )
    read_own = each(
        lambda a, b, c: a[span:] + single(b, spread(c)), from_value, read_write, inv_value
    )
    tail = each(lambda a, b: jnp.exp(a - b), last, middle)
    write_end = each(lambda a, b: a * b, write, tail)
    key_end = each(lambda a, b: a * b, keys, tail)
    low = each(lambda a, b: single(a.T, b) * wide_mask, inv_remove, write_end)

    def gained(a, b, c, d):
        full = (
            single(jnp.concatenate([a, b], axis=0).T, jnp.concatenate([c, d], axis=0)) * wide_mask
        )
        return sum(full[h * head_width : (h + 1) * head_width] for h in range(per_group))

    added = each(gained, inv_value, value, write_end, key_end)
    kept = [jnp.exp(x) for x in last]
    return read_map, read_own, low, kept, added, spread


def mixed_rows(head_width, rows, state, refs, mask):
    map_ref, own_ref, recept_ref, key_ref, value_ref, gate_ref, gain_ref, self_ref = refs
    groups = [slice(g * LANES, (g + 1) * LANES) for g in range(map_ref.shape[1] // LANES)]
    copies = LANES // head_width

    def spread(x):
        return jnp.concatenate([x.astype(jnp.bfloat16)] * copies, axis=0) * mask

    read = [
        own_ref[rows, cols] + single(map_ref[rows, cols], spread(state[g]), NT)
        for g, cols in enumerate(groups)
    ]
    own = [
        head_sum(
            recept_ref[rows, cols].astype(jnp.float32)
            * key_ref[rows, cols].astype(jnp.float32)
            * self_ref[:, cols],
            mask,
        )
        * value_ref[rows, cols].astype(jnp.float32)
        for cols in groups
    ]
    off = [x - head_sum(x, mask) * (1.0 / head_width) for x in read]
    width = [single(x * x, mask) * (1.0 / head_width) for x in off]
    return [
        (
            (off[g] * lax.rsqrt(width[g] + GROUP_EPS) * gain_ref[:, cols] + own[g])
            * gate_ref[rows, cols].astype(jnp.float32)
        ).astype(jnp.bfloat16)
        for g, cols in enumerate(groups)
    ]


class Inputs(typing.NamedTuple):
    recept: typing.Any
    key: typing.Any
    value: typing.Any
    decay: typing.Any
    rate: typing.Any
    offset: typing.Any
    decay_bias: typing.Any
    rate_bias: typing.Any
    gain: typing.Any
    self_weight: typing.Any
    norm_gain: typing.Any
    share: typing.Any
    output_gate: typing.Any
    out_weight: typing.Any
    residual: typing.Any
    gate: typing.Any
    up: typing.Any
    down: typing.Any


class InnerSems(typing.NamedTuple):
    load: typing.Any
    state_send: typing.Any
    state_recv: typing.Any
    sum_core_send: typing.Any
    sum_core_recv: typing.Any
    sum_chip_send: typing.Any
    sum_chip_recv: typing.Any
    core_send: typing.Any
    core_recv: typing.Any
    chip_send: typing.Any
    chip_recv: typing.Any
    swap_send: typing.Any
    swap_recv: typing.Any
    pass_send: typing.Any
    pass_recv: typing.Any
    weight_load: typing.Any
    share_send: typing.Any
    share_recv: typing.Any


class Flows(typing.NamedTuple):
    blocks: typing.Any
    result: typing.Any
    from_right: typing.Any
    from_left: typing.Any
    to_left: typing.Any
    to_right: typing.Any


class FlowSems(typing.NamedTuple):
    gather_send: typing.Any
    gather_recv: typing.Any
    flow_send: typing.Any
    flow_recv: typing.Any


def layer_kernel(names, head_width, pieces, lag, *all_refs):
    ref = types.SimpleNamespace(**dict(zip(names, all_refs, strict=True)))
    with_experts = hasattr(ref, "out")
    place, count = lax.axis_index("sp"), lax.axis_size("sp")
    near, far, cross = tp_peers()
    mine = lax.axis_index("tp")
    ahead, behind = peer(sp=(place + 1) % count), peer(sp=(place + count - 1) % count)
    has_left, has_right = place > 0, place < count - 1
    length, width = ref.recept_all.shape
    groups = [slice(g * LANES, (g + 1) * LANES) for g in range(width // LANES)]
    rows = ref.residual.shape[0]
    size = rows // pieces
    mask = block_mask(head_width).astype(jnp.bfloat16)

    weights = Gather(
        (ref.gate, ref.up, ref.down),
        (ref.gates, ref.ups, ref.downs),
        tuple(getattr(ref, name) for name in InnerSems._fields[7:16]),
    )
    shares = Spread(ref.share, ref.shares, ref.share_send, ref.share_recv)
    barrier = pltpu.get_barrier_semaphore()
    for device in (weights.near, weights.far, weights.twin):
        greet(barrier, device)
    pl.semaphore_wait(barrier, 3 + shares.greet(barrier))
    weights.begin()
    shares.begin()
    loads = [
        pltpu.make_async_copy(source, held, ref.load.at[k])
        for k, (source, held) in enumerate(
            (
                (ref.recept, ref.recept_all),
                (ref.key, ref.key_all),
                (ref.value, ref.value_all),
                (ref.decay, ref.decay_all),
                (ref.rate, ref.rate_all),
                (ref.output_gate, ref.output_gate_all),
                (ref.out_weight, ref.out_weight_all),
                (ref.residual, ref.residual_all),
            )
        )
    ]
    for load in loads:
        load.start()
    for load in loads[:5]:
        load.wait()

    full_lanes = lax.broadcasted_iota(jnp.int32, ref.transit.shape, 1) % head_width
    full_rows = lax.broadcasted_iota(jnp.int32, ref.transit.shape, 0)
    ref.transit[...] = jnp.where(full_lanes == full_rows, 1.0, 0.0)
    ref.added[...] = jnp.zeros_like(ref.added)
    chunk_refs = (ref.recept_all, ref.key_all, ref.value_all, ref.decay_all, ref.rate_all, ref.decay_bias, ref.rate_bias)
    per_step = 2

    def chunk_step(step, carry):
        cells, offsets = [], []
        span = per_step * head_width
        by_head = ref.offset[:, pl.ds(pl.multiple_of(step * span, span), span)].T
        for chunk in range(per_step):
            own_offset = by_head[chunk * head_width : (chunk + 1) * head_width]
            offsets += [own_offset] * len(groups)
            first = pl.multiple_of((step * per_step + chunk) * head_width, head_width)
            cells += [(pl.ds(first, head_width), cols) for cols in groups]
        read_map, read_own, low, kept, added, spread = chunk_cells(
            head_width, chunk_refs, cells, offsets
        )
        for k, at in enumerate(cells):
            cols = at[1]
            held_transit, held_added = ref.transit[:, cols], ref.added[:, cols]
            ref.map[at] = single(read_map[k], spread(held_transit), NT).astype(jnp.bfloat16)
            ref.own[at] = read_own[k] + single(read_map[k], spread(held_added), NT)
            held = jnp.concatenate([held_transit, held_added], axis=0)
            moved = held * kept[k] + single(held, low[k])
            ref.transit[:, cols] = moved[:head_width]
            ref.added[:, cols] = moved[head_width:] + added[k]

        for index in range(2):
            pl.when(step == index + 1)(functools.partial(weights.arrive_chip, index))

        return carry

    lax.fori_loop(0, length // (per_step * head_width), chunk_step, 0)

    state_ref, onward_ref = ref.state, ref.onward

    def state_copy(group):
        return remote(
            onward_ref.at[group],
            state_ref.at[group],
            ref.state_send.at[group],
            ref.state_recv.at[group],
            ahead,
        )

    @pl.when(place == 0)
    def _():
        for group, cols in enumerate(groups):
            state_ref[group] = jnp.zeros_like(state_ref[group])
            onward_ref[group] = ref.added[:, cols]
            state_copy(group).start()

    weights.arrive_chip(2)

    @pl.when(has_left)
    def _():
        for group, cols in enumerate(groups):
            state_copy(group).wait_recv()

            @pl.when(has_right)
            def _(group=group, cols=cols):
                onward_ref[group] = ref.added[:, cols] + product(
                    halves(state_ref[group]), spread_blocks(ref.transit[:, cols], mask), NN
                )
                state_copy(group).start()

    weights.arrive_chip(3)
    weights.arrive_swap(0)
    weights.arrive_swap(1)
    for load in loads[5:]:
        load.wait()

    mixed_refs = (ref.map, ref.own, ref.recept_all, ref.key_all, ref.value_all, ref.output_gate_all, ref.gain, ref.self_weight)
    core_out, core_in = ref.core_out, ref.core_in
    chip_out, chip_in = ref.chip_out, ref.chip_in

    def partial(owner, part):
        at = pl.ds(pl.multiple_of(owner * rows + part * size, size), size)
        mixed = mixed_rows(head_width, at, state_ref, mixed_refs, mask)
        return single(jnp.concatenate(mixed, axis=1), ref.out_weight_all[...])

    def core_copy(which, part):
        slot = which * pieces + part
        return remote(
            core_out.at[slot],
            core_in.at[slot],
            ref.sum_core_send.at[slot],
            ref.sum_core_recv.at[slot],
            weights.near,
        )

    def chip_copy(part):
        return remote(
            chip_out.at[part],
            chip_in.at[part],
            ref.sum_chip_send.at[part],
            ref.sum_chip_recv.at[part],
            weights.far,
        )

    stream_ref, features_ref = ref.stream, ref.features
    for part in range(pieces):
        core_out[part] = partial(cross, part)
        core_copy(0, part).start()
        own = partial(far, part)
        core_copy(0, part).wait_recv()
        chip_out[part] = (own + core_in[part]).astype(jnp.bfloat16)
        chip_copy(part).start()
        if part == 0:
            weights.begin_late()
    weights.arrive_chip(4)
    weights.arrive_chip(5)

    def sum_own(part):
        at = slice(part * size, (part + 1) * size)
        core_out[pieces + part] = partial(near, part)
        core_copy(1, part).start()
        own = partial(mine, part)
        core_copy(1, part).wait_recv()
        stream_ref[at] = (
            ref.residual_all[at].astype(jnp.float32) + own + core_in[pieces + part]
        )

    def pass_late():
        weights.arrive_swap(4)
        weights.arrive_swap(5)

    def finish_stream(part):
        sum_own(part)
        if part == pieces - 1:
            weights.arrive_chip(LATE)
            weights.arrive_swap(2)
            weights.arrive_swap(3)
        at = slice(part * size, (part + 1) * size)
        chip_copy(part).wait_recv()
        stream = stream_ref[at] + chip_in[part].astype(jnp.float32)
        stream_ref[at] = stream
        features_ref[at] = (
            stream
            * lax.rsqrt(jnp.mean(stream * stream, axis=-1, keepdims=True) + NORM_EPS)
            * ref.norm_gain[...]
        ).astype(jnp.bfloat16)

    def drain_first():
        @pl.when(has_right)
        def _():
            for group in range(len(groups)):
                state_copy(group).wait_send()

        for part in range(pieces):
            core_copy(0, part).wait_send()
            core_copy(1, part).wait_send()
            chip_copy(part).wait_send()
        weights.drain()

    if not with_experts:
        for part in range(pieces):
            finish_stream(part)
        pass_late()
        weights.arrive_rest()
        shares.end()
        drain_first()
        return

    blocks, result, from_right, from_left, to_left, to_right = (getattr(ref, name) for name in Flows._fields)

    def gather_copy(source, block, piece, part, way):
        return remote(
            source,
            blocks.at[block, piece, part],
            ref.gather_send.at[way, block, piece, part],
            ref.gather_recv.at[block, piece, part],
            ahead if way else behind,
        )

    def sum_copy(block, piece, part, way):
        out, into = (to_right, from_left) if way else (to_left, from_right)
        return remote(
            out.at[block, piece, part],
            into.at[block, piece, part],
            ref.flow_send.at[way, block, piece, part],
            ref.flow_recv.at[way, block, piece, part],
            ahead if way else behind,
        )

    parts = blocks.shape[2]
    fine = blocks.shape[3]

    def send_own(piece, way):
        for part in range(parts):
            own_features = features_ref.at[pl.ds(piece * size + part * fine, fine)]
            gather_copy(own_features, place, piece, part, way).start()

    finish_stream(0)
    pl.when(has_left)(lambda: send_own(0, 0))
    pl.when(has_right)(lambda: send_own(0, 1))
    finish_stream(1)
    pl.when(has_left & (place == count - 1))(lambda: send_own(1, 0))
    pl.when(has_right & (place == 0))(lambda: send_own(1, 1))

    def apply(features, block, piece):
        total = None
        for j in range(ref.gates.shape[0]):
            gated = single(features, ref.gates[j])
            upward = single(features, ref.ups[j])
            term = single(jax.nn.silu(gated) * upward, ref.downs[j])
            total = term if total is None else total + term
        own = ref.shares[block, pl.ds(pl.multiple_of(piece * size, size), size)]
        lanes = lax.broadcasted_iota(jnp.int32, own.shape, 1)
        share = jnp.sum(jnp.where(lanes == place, own, 0.0), axis=1, keepdims=True)
        result[block, piece] = (total * share).reshape(parts, fine, total.shape[1])

    def slot(time, carry):
        arrivals = []
        for way, before in ((1, place), (0, count - 1 - place)):
            step = 1 if way else -1
            far = 0 if way else count - 1
            first = time < before
            block = jnp.where(first, place - step * (1 + time), far + step * (time - before))
            piece = jnp.where(first, 0, 1)
            arrivals.append((way, block, piece, time < 2 * before, time == 2 * before - 1))

        for way, block, piece, there, final in arrivals:
            onward = has_right if way else has_left

            @pl.when(there)
            def _(way=way, block=block, piece=piece, onward=onward, final=final):
                for part in range(parts):
                    landed = blocks.at[block, piece, part]
                    gather_copy(landed, block, piece, part, way).wait_recv()
                    pl.when(onward)(
                        lambda: gather_copy(landed, block, piece, part, way).start()
                    )
                pl.when(onward & final)(lambda: send_own(1, way))

        @pl.when(time == 0)
        def _():
            pass_late()
            weights.arrive_rest()
            shares.end()

        own = time - 2 * (count - 1)

        @pl.when((own >= 0) & (own < pieces))
        def _():
            at = pl.ds(pl.multiple_of(own * size, size), size)
            apply(features_ref[at], place, own)

        for way, block, piece, there, final in arrivals:

            @pl.when(there)
            def _(block=block, piece=piece):
                features = blocks[block, piece]
                apply(features.reshape(size, features.shape[2]), block, piece)

        for way, hops, more, into, out in (
            (0, count - 1 - place, has_right, from_right, to_left),
            (1, place, has_left, from_left, to_right),
        ):
            turn = time - lag * hops
            first = turn < count - 1
            offset = jnp.where(first, count - 2 - turn, turn - (count - 1))
            block = count - 1 - offset if way else offset
            piece = jnp.where(first, 0, 1)
            passed = block - place if way else place - block
            valid = (turn >= 0) & (turn < 2 * (count - 1)) & (passed >= 0)

            for part in range(parts):

                @pl.when(valid & more)
                def _(way=way, block=block, piece=piece, part=part, into=into):
                    sum_copy(block, piece, part, way).wait_recv()

                @pl.when(valid & more & (passed > 0))
                def _(block=block, piece=piece, part=part, into=into, out=out):
                    total = result[block, piece, part] + into[block, piece, part].astype(
                        jnp.float32
                    )
                    out[block, piece, part] = total.astype(jnp.bfloat16)

                @pl.when(valid & jnp.logical_not(more))
                def _(block=block, piece=piece, part=part, out=out):
                    out[block, piece, part] = result[block, piece, part].astype(jnp.bfloat16)

                @pl.when(valid & (passed > 0))
                def _(way=way, block=block, piece=piece, part=part):
                    sum_copy(block, piece, part, way).start()

        return carry

    lax.fori_loop(0, (2 + lag) * (count - 1), slot, 0)
    for piece in range(pieces):
        at = slice(piece * size, (piece + 1) * size)
        shape = (size, stream_ref.shape[1])
        stream_ref[at] = stream_ref[at] + result[place, piece].reshape(shape)
        for there, into in ((has_right, from_right), (has_left, from_left)):

            @pl.when(there)
            def _(at=at, into=into, piece=piece):
                stream_ref[at] = stream_ref[at] + into[place, piece].reshape(shape).astype(
                    jnp.float32
                )

        ref.out[at] = stream_ref[at].astype(jnp.bfloat16)

    def drain(block, carry):
        for piece in range(pieces):
            for part in range(parts):
                landed = blocks.at[block, piece, part]
                for way, gathers, sums in (
                    (0, has_left & (block >= place), has_left & (block < place)),
                    (1, has_right & (block <= place), has_right & (block > place)),
                ):
                    pl.when(gathers)(
                        lambda: gather_copy(landed, block, piece, part, way).wait_send()
                    )
                    pl.when(sums)(lambda: sum_copy(block, piece, part, way).wait_send())
        return carry

    lax.fori_loop(0, count, drain, 0)
    drain_first()


def shares_of(routed_expert_index, routed_expert_weight, experts):
    ids = jnp.arange(experts + -experts % 128, dtype=jnp.int32)
    return jnp.sum(
        jnp.where(
            routed_expert_index[:, :, None] == ids, routed_expert_weight[:, :, None], 0.0
        ),
        axis=1,
    )


def experts_by_collectives(features, stream, shares, gates, ups, downs):
    features = lax.all_gather(features, "sp", axis=0, tiled=True)
    shares = shares.reshape(-1, shares.shape[-1])
    place = lax.axis_index("sp")
    lanes = jnp.arange(shares.shape[1], dtype=jnp.int32)
    share = jnp.sum(jnp.where(lanes[None, :] == place, shares, 0.0), axis=1, keepdims=True)
    depth = features.shape[1]

    def some_rows(operands):
        features, share = operands
        total = None
        for gate, up, down in zip(gates, ups, downs):
            for j in range(gate.shape[0]):
                gated = jnp.dot(features, gate[j], preferred_element_type=jnp.float32)
                upward = jnp.dot(features, up[j], preferred_element_type=jnp.float32)
                hidden = (jax.nn.silu(gated) * upward).astype(jnp.bfloat16)
                term = jnp.dot(hidden, down[j], preferred_element_type=jnp.float32)
                total = term if total is None else total + term
        return (total * share).astype(jnp.bfloat16)

    rows = stream.shape[0]
    total = lax.map(
        some_rows, (features.reshape(-1, rows, depth), share.reshape(-1, rows, 1))
    ).reshape(-1, depth)
    weighted = lax.psum_scatter(total, "sp", scatter_dimension=0, tiled=True)
    return (stream + weighted.astype(jnp.float32)).astype(jnp.bfloat16)


PIECES = 2
PARTS = 2
LAG = 1


def local(
    recept,
    key_input,
    value_input,
    output_gate_input,
    decay_input_part,
    correction_rate_input,
    head_decay_offset,
    decay_fixed_bias,
    correction_rate_bias,
    head_norm_gain,
    self_term_weight,
    output_weight_matrix,
    residual,
    feedforward_norm_gain,
    routed_expert_index,
    routed_expert_weight,
    gate_weight_experts,
    up_weight_experts,
    down_weight_experts,
):
    count = lax.axis_size("sp")
    experts = gate_weight_experts.shape[0] * count
    assert lax.axis_size("tp") == 4 and lax.axis_size("grp") == 2
    assert gate_weight_experts.shape[0] == 1
    length, width = recept.shape
    heads = head_decay_offset.shape[1]
    head_width = width // heads
    own_rows, depth = residual.shape
    shares = shares_of(routed_expert_index, routed_expert_weight, experts)
    gate, up, down = gate_weight_experts[0], up_weight_experts[0], down_weight_experts[0]
    groups = width // LANES
    half = own_rows // PIECES
    dma = pltpu.SemaphoreType.DMA
    single_bf, single_f32 = jnp.bfloat16, jnp.float32

    def like(x):
        return (x.shape, x.dtype)

    kept = dict(
        stream=((own_rows, depth), single_f32),
        features=((own_rows, depth), single_bf),
        shares=((count, *shares.shape), single_f32),
        gates=((4, *gate.shape), gate.dtype),
        ups=((4, *up.shape), up.dtype),
        downs=((4, *down.shape), down.dtype),
    )
    sums = ((2 * PIECES, half, depth), single_f32)
    chips = ((PIECES, half, depth), single_bf)
    states = ((groups, head_width, LANES), single_f32)
    inner = dict(
        recept_all=like(recept),
        key_all=like(key_input),
        value_all=like(value_input),
        decay_all=like(decay_input_part),
        rate_all=like(correction_rate_input),
        output_gate_all=like(output_gate_input),
        out_weight_all=like(output_weight_matrix),
        residual_all=like(residual),
        map=((length, width), single_bf),
        own=((length, width), single_f32),
        transit=((head_width, width), single_f32),
        added=((head_width, width), single_f32),
        state=states,
        onward=states,
        core_out=sums,
        core_in=sums,
        chip_out=chips,
        chip_in=chips,
    )
    sems = [(8,), (groups,), (groups,)] + [(2 * PIECES,)] * 2 + [(PIECES,)] * 2
    portions = len(PORTIONS)
    sems += [(3,)] * 2 + [(portions,)] * 4 + [(2 * portions,)] * 2 + [(3,), (count,), (count,)]
    inner_sems = dict(zip(InnerSems._fields, sems, strict=True))
    with_experts = count <= 4
    scratch, outs = dict(inner), dict(kept)
    if with_experts:
        flow = ((count, PIECES, PARTS, half // PARTS, depth), single_bf)
        scratch = kept | inner
        scratch |= {name: flow for name in Flows._fields} | dict(result=(flow[0], single_f32))
        outs = dict(out=((own_rows, depth), single_bf))
        both = (2, count, PIECES, PARTS)
        inner_sems |= dict(zip(FlowSems._fields, (both, both[1:], both, both), strict=True))
    names = [*Inputs._fields, *outs, *scratch, *inner_sems]
    anywhere = pl.BlockSpec(memory_space=pl.ANY)
    in_vmem = pl.BlockSpec(memory_space=pltpu.VMEM)
    results = pl.pallas_call(
        functools.partial(layer_kernel, names, head_width, PIECES, LAG),
        in_specs=[anywhere] * 5 + [in_vmem] * 7 + [anywhere] * 6,
        out_specs=[in_vmem] * len(outs),
        out_shape=[jax.ShapeDtypeStruct(*spec) for spec in outs.values()],
        scratch_shapes=[pltpu.VMEM(*spec) for spec in scratch.values()]
        + [dma(shape) for shape in inner_sems.values()],
        compiler_params=pltpu.CompilerParams(
            collective_id=0, has_side_effects=True, vmem_limit_bytes=VMEM_LIMIT
        ),
        cost_estimate=pl.CostEstimate(
            flops=30_000_000_000, bytes_accessed=40 * length * width, transcendentals=0
        ),
        name="layer",
    )(
        recept,
        key_input,
        value_input,
        decay_input_part,
        correction_rate_input,
        head_decay_offset.T,
        decay_fixed_bias[None],
        correction_rate_bias[None],
        head_norm_gain[None],
        self_term_weight[None],
        feedforward_norm_gain[None],
        shares,
        output_gate_input,
        output_weight_matrix,
        residual,
        gate,
        up,
        down,
    )
    if with_experts:
        return results[0]
    stream, features, all_shares, *full = results
    return experts_by_collectives(features, stream, all_shares, *((each,) for each in full))


def solution(mesh):
    return jax.shard_map(
        local,
        mesh=mesh,
        in_specs=(
            P(("grp", "sp"), "tp"),
            P(("grp", "sp"), "tp"),
            P(("grp", "sp"), "tp"),
            P(("grp", "sp"), "tp"),
            P(("grp", "sp"), "tp"),
            P(("grp", "sp"), "tp"),
            P(("grp", "sp"), "tp"),
            P("tp"),
            P("tp"),
            P("tp"),
            P("tp"),
            P("tp", None),
            P(("grp", "sp", "tp"), None),
            P(),
            P(("grp", "sp", "tp"), None),
            P(("grp", "sp", "tp"), None),
            P("sp", None, "tp"),
            P("sp", None, "tp"),
            P("sp", "tp", None),
        ),
        out_specs=P(("grp", "sp", "tp"), None),
        check_vma=False,
    )
```

```python
import functools
import types
import typing

import jax
import jax.numpy as jnp
from jax import lax
from jax.experimental import pallas as pl
from jax.experimental.pallas import tpu as pltpu
from jax.sharding import PartitionSpec as P

SPAN = 64
LANES = 256
GROUP_EPS = 0.00064
NORM_EPS = 1e-06
NN = (((1,), (0,)), ((), ()))
NT = (((1,), (1,)), ((), ()))
MESH = pl.DeviceIdType.MESH
VMEM_LIMIT = 60 * 1024 * 1024


def peer(**coords):
    return tuple(coords.get(name, lax.axis_index(name)) for name in ("grp", "sp", "tp"))


def tp_peers():
    place = lax.axis_index("tp")
    chip, core = place // 2, place % 2
    return 2 * chip + 1 - core, 2 * (1 - chip) + core, 2 * (1 - chip) + 1 - core


def remote(src, dst, send_sem, recv_sem, device):
    return pltpu.make_async_remote_copy(
        src_ref=src,
        dst_ref=dst,
        send_sem=send_sem,
        recv_sem=recv_sem,
        device_id=device,
        device_id_type=MESH,
    )


def greet(barrier, device):
    pl.semaphore_signal(barrier, inc=1, device_id=device, device_id_type=MESH)


def halves(x):
    high = x.astype(jnp.bfloat16)
    return high, (x - high.astype(jnp.float32)).astype(jnp.bfloat16)


def product(left, right, dims):
    def dot(a, b):
        return lax.dot_general(a, b, dims, preferred_element_type=jnp.float32)

    return dot(left[0], right[0]) + (dot(left[1], right[0]) + dot(left[0], right[1]))


def block_mask(head_width):
    rows = lax.broadcasted_iota(jnp.int32, (LANES, LANES), 0) // head_width
    lanes = lax.broadcasted_iota(jnp.int32, (LANES, LANES), 1) // head_width
    return jnp.where(rows == lanes, 1.0, 0.0)


def spread_blocks(x, mask):
    copies = LANES // x.shape[0]
    return tuple(jnp.concatenate([part] * copies, axis=0) * mask for part in halves(x))


def head_sum(x, mask):
    high, low = halves(x)
    return lax.dot_general(
        high, mask, NN, preferred_element_type=jnp.float32
    ) + lax.dot_general(low, mask, NN, preferred_element_type=jnp.float32)


PORTIONS = ((0, 0, 4), (0, 4, 4), (1, 0, 4), (1, 4, 4), (2, 0, 4), (2, 4, 2), (2, 6, 2))
LATE = len(PORTIONS) - 1


class Gather:
    def __init__(self, own, full, sems):
        self.own, self.full = own, full
        (
            self.core_send,
            self.core_recv,
            self.chip_send,
            self.chip_recv,
            self.swap_send,
            self.swap_recv,
            self.pass_send,
            self.pass_recv,
            self.load,
        ) = sems
        near, far, _ = tp_peers()
        self.group = lax.axis_index("grp")
        self.near, self.far = peer(tp=near), peer(tp=far)
        self.twin = peer(grp=1 - self.group)

    def portion(self, refs, index, which, slot=None):
        k, first, size = PORTIONS[index]
        ref = refs[k]
        rows = ref.shape[-2] // 2
        unit = rows // 8
        start = pl.multiple_of(which * rows + first * unit, unit)
        at = pl.ds(start, size * unit)
        return ref.at[at] if slot is None else ref.at[slot, at]

    def core_copy(self, k):
        return remote(
            self.own[k], self.full[k].at[1], self.core_send.at[k], self.core_recv.at[k], self.near
        )

    def chip_copy(self, index):
        return remote(
            self.portion(self.own, index, self.group),
            self.portion(self.full, index, self.group, 2),
            self.chip_send.at[index],
            self.chip_recv.at[index],
            self.far,
        )

    def swap_copy(self, index, which):
        piece = self.portion(self.full, index, which, 2)
        return remote(
            piece, piece, self.swap_send.at[index], self.swap_recv.at[index], self.twin
        )

    def pass_copy(self, index, swapped):
        which = 1 - self.group if swapped else self.group
        slot = 2 * index + swapped
        return remote(
            self.portion(self.full, index, which, 2),
            self.portion(self.full, index, which, 3),
            self.pass_send.at[slot],
            self.pass_recv.at[slot],
            self.near,
        )

    def load_copy(self, k):
        return pltpu.make_async_copy(self.own[k], self.full[k].at[0], self.load.at[k])

    def begin(self):
        for index in range(LATE):
            self.chip_copy(index).start()
        for k in range(3):
            self.core_copy(k).start()
            self.load_copy(k).start()

    def begin_late(self):
        self.chip_copy(LATE).start()

    def arrive_chip(self, index):
        self.chip_copy(index).wait_recv()
        self.swap_copy(index, self.group).start()
        self.pass_copy(index, 0).start()

    def arrive_swap(self, index):
        self.swap_copy(index, 1 - self.group).wait_recv()
        self.pass_copy(index, 1).start()

    def arrive_rest(self):
        self.arrive_swap(LATE)
        for k in range(3):
            self.load_copy(k).wait()
            self.core_copy(k).wait_recv()
        for index in range(len(PORTIONS)):
            for swapped in range(2):
                self.pass_copy(index, swapped).wait_recv()

    def drain(self):
        for k in range(3):
            self.core_copy(k).wait_send()
        for index in range(len(PORTIONS)):
            self.chip_copy(index).wait_send()
            self.swap_copy(index, self.group).wait_send()
            for swapped in range(2):
                self.pass_copy(index, swapped).wait_send()


class Spread:
    def __init__(self, own, full, send, recv):
        self.own, self.full, self.send, self.recv = own, full, send, recv
        self.count = lax.axis_size("sp")
        self.place = lax.axis_index("sp")

    def greet(self, barrier):
        def one(ahead, carry):
            greet(barrier, peer(sp=(self.place + ahead) % self.count))
            return carry

        lax.fori_loop(1, self.count, one, 0)
        return self.count - 1

    def copy(self, ahead):
        return remote(
            self.own,
            self.full.at[self.place],
            self.send.at[ahead - 1],
            self.recv.at[self.place],
            peer(sp=(self.place + ahead) % self.count),
        )

    def arrival(self, ahead):
        source = (self.place + self.count - ahead) % self.count
        return remote(
            self.own,
            self.full.at[source],
            self.send.at[ahead - 1],
            self.recv.at[source],
            peer(sp=source),
        )

    def begin(self):
        self.full[self.place] = self.own[...]

        def one(ahead, carry):
            self.copy(ahead).start()
            return carry

        lax.fori_loop(1, self.count, one, 0)

    def end(self):
        def one(ahead, carry):
            self.copy(ahead).wait_send()
            self.arrival(ahead).wait_recv()
            return carry

        lax.fori_loop(1, self.count, one, 0)


def single(left, right, dims=NN):
    return lax.dot_general(
        left.astype(jnp.bfloat16),
        right.astype(jnp.bfloat16),
        dims,
        preferred_element_type=jnp.float32,
    )


def chunk_cells(head_width, refs, cells, offsets):
    recept_ref, key_ref, value_ref, decay_ref, rate_ref, decay_bias, rate_bias = refs
    span = head_width
    per_group = LANES // head_width
    wide_mask = block_mask(head_width)
    mask = wide_mask.astype(jnp.bfloat16)
    times = lax.broadcasted_iota(jnp.int32, (span, LANES), 0)
    lanes = lax.broadcasted_iota(jnp.int32, (span, LANES), 1)
    earlier = lanes % head_width
    strict = times > earlier
    within = times >= earlier
    eye = jnp.where(times == earlier, 1.0, 0.0)
    tri_rows = lax.broadcasted_iota(jnp.int32, (span, 3 * span), 0)
    tri_lanes = lax.broadcasted_iota(jnp.int32, (span, 3 * span), 1) % span
    tri = jnp.where(tri_rows >= tri_lanes, 1.0, 0.0).astype(jnp.bfloat16)

    def spread(x):
        return jnp.concatenate([x.astype(jnp.bfloat16)] * per_group, axis=0) * mask

    def each(step, *lists):
        return [step(*values) for values in zip(*lists)]

    def load(ref):
        return [ref[rows, cols].astype(jnp.float32) for rows, cols in cells]

    recept, key, value = load(recept_ref), load(key_ref), load(value_ref)

    def decays(cell, extra, by_head):
        cols = cell[1]
        offset = jnp.zeros((span, LANES), jnp.float32)
        for head in range(per_group):
            column = cols.start // head_width + head
            offset = jnp.where(
                lanes // head_width == head, by_head[:, column : column + 1], offset
            )
        return offset - 0.6065306597126334 / (1.0 + jnp.exp(-(decay_bias[:, cols] + extra)))

    decay = each(decays, cells, load(decay_ref), offsets)
    rate = each(
        lambda cell, extra: 1.0 / (1.0 + jnp.exp(-(rate_bias[:, cell[1]] + extra))),
        cells,
        load(rate_ref),
    )
    norm = each(lambda k: single(k * k, mask), key)
    unit = each(lambda k, n: k * lax.rsqrt(n + NORM_EPS), key, norm)

    def cumulative(d):
        one, rest = halves(d)
        third = (d - one.astype(jnp.float32) - rest.astype(jnp.float32)).astype(jnp.bfloat16)
        return single(tri, jnp.concatenate([third, rest, one], axis=0))

    cumul = each(cumulative, decay)
    middle = [c[span // 2 : span // 2 + 1] for c in cumul]
    last = [c[span - 1 : span] for c in cumul]
    center = each(lambda c, m: c - m, cumul, middle)
    grow = each(lambda c: jnp.exp(-c), center)
    remove = each(lambda u, c, d: -u * jnp.exp(c - d), unit, center, decay)
    reads = each(lambda r, c: r * jnp.exp(c), recept, center)
    write = each(lambda u, r, g: u * r * g, unit, rate, grow)
    keys = each(lambda k, g: k * g, key, grow)
    left = each(
        lambda a, b: jnp.concatenate([a, b], axis=0).astype(jnp.bfloat16), remove, reads
    )
    by_write = each(lambda a, b: single(a, spread(b), NT), left, write)
    by_key = each(lambda a, b: single(a, spread(b), NT), left, keys)
    remove_write = [jnp.where(strict, x[:span], 0.0) for x in by_write]
    read_write = [jnp.where(within, x[span:], 0.0).astype(jnp.bfloat16) for x in by_write]
    key_rows = [
        jnp.concatenate(
            [jnp.where(strict, x[:span], 0.0), jnp.where(within, x[span:], 0.0)], axis=0
        )
        for x in by_key
    ]
    from_value = each(
        lambda a, b: sum(single(part, spread(b)) for part in halves(a)), key_rows, value
    )
    inverse = [eye + jnp.where(times // 2 == earlier // 2, x, 0.0) for x in remove_write]
    size = 2
    while size < span:
        joint = (times // (2 * size) == earlier // (2 * size)) & (
            times // size != earlier // size
        )
        step = each(
            lambda a, b: single(a, spread(jnp.where(joint, b, 0.0))), inverse, remove_write
        )
        inverse = each(lambda a, b: b + single(a, spread(b)), step, inverse)
        size *= 2
    start = [jnp.exp(m) for m in middle]
    inverse = [x.astype(jnp.bfloat16) for x in inverse]

    def applied(a, b):
        return sum(single(a, part) for part in spread_blocks(b, mask))

    inv_remove = each(lambda a, b, c: applied(a, b) * c, inverse, remove, start)
    inv_value = each(lambda a, b: applied(a, b[:span]), inverse, from_value)
    read_map = each(
        lambda a, b, c, d: a * b + single(c, spread(d)), reads, start, read_write, inv_remove
    )
    read_own = each(
        lambda a, b, c: a[span:] + single(b, spread(c)), from_value, read_write, inv_value
    )
    tail = each(lambda a, b: jnp.exp(a - b), last, middle)
    write_end = each(lambda a, b: a * b, write, tail)
    key_end = each(lambda a, b: a * b, keys, tail)
    low = each(lambda a, b: single(a.T, b) * wide_mask, inv_remove, write_end)

    def gained(a, b, c, d):
        full = (
            single(jnp.concatenate([a, b], axis=0).T, jnp.concatenate([c, d], axis=0)) * wide_mask
        )
        return sum(full[h * head_width : (h + 1) * head_width] for h in range(per_group))

    added = each(gained, inv_value, value, write_end, key_end)
    kept = [jnp.exp(x) for x in last]
    return read_map, read_own, low, kept, added, spread


def mixed_rows(head_width, rows, state, refs, mask):
    map_ref, own_ref, recept_ref, key_ref, value_ref, gate_ref, gain_ref, self_ref = refs
    groups = [slice(g * LANES, (g + 1) * LANES) for g in range(map_ref.shape[1] // LANES)]
    copies = LANES // head_width

    def spread(x):
        return jnp.concatenate([x.astype(jnp.bfloat16)] * copies, axis=0) * mask

    read = [
        own_ref[rows, cols] + single(map_ref[rows, cols], spread(state[g]), NT)
        for g, cols in enumerate(groups)
    ]
    own = [
        head_sum(
            recept_ref[rows, cols].astype(jnp.float32)
            * key_ref[rows, cols].astype(jnp.float32)
            * self_ref[:, cols],
            mask,
        )
        * value_ref[rows, cols].astype(jnp.float32)
        for cols in groups
    ]
    off = [x - head_sum(x, mask) * (1.0 / head_width) for x in read]
    width = [single(x * x, mask) * (1.0 / head_width) for x in off]
    return [
        (
            (off[g] * lax.rsqrt(width[g] + GROUP_EPS) * gain_ref[:, cols] + own[g])
            * gate_ref[rows, cols].astype(jnp.float32)
        ).astype(jnp.bfloat16)
        for g, cols in enumerate(groups)
    ]


class Inputs(typing.NamedTuple):
    recept: typing.Any
    key: typing.Any
    value: typing.Any
    decay: typing.Any
    rate: typing.Any
    offset: typing.Any
    decay_bias: typing.Any
    rate_bias: typing.Any
    gain: typing.Any
    self_weight: typing.Any
    norm_gain: typing.Any
    route_index: typing.Any
    route_weight: typing.Any
    output_gate: typing.Any
    out_weight: typing.Any
    residual: typing.Any
    gate: typing.Any
    up: typing.Any
    down: typing.Any


class InnerSems(typing.NamedTuple):
    load: typing.Any
    state_send: typing.Any
    state_recv: typing.Any
    sum_core_send: typing.Any
    sum_core_recv: typing.Any
    sum_chip_send: typing.Any
    sum_chip_recv: typing.Any
    core_send: typing.Any
    core_recv: typing.Any
    chip_send: typing.Any
    chip_recv: typing.Any
    swap_send: typing.Any
    swap_recv: typing.Any
    pass_send: typing.Any
    pass_recv: typing.Any
    weight_load: typing.Any
    share_send: typing.Any
    share_recv: typing.Any


class Flows(typing.NamedTuple):
    blocks: typing.Any
    result: typing.Any
    from_right: typing.Any
    from_left: typing.Any
    to_left: typing.Any
    to_right: typing.Any


class FlowSems(typing.NamedTuple):
    gather_send: typing.Any
    gather_recv: typing.Any
    flow_send: typing.Any
    flow_recv: typing.Any


def layer_kernel(names, head_width, pieces, lag, *all_refs):
    ref = types.SimpleNamespace(**dict(zip(names, all_refs, strict=True)))
    with_experts = hasattr(ref, "out")
    place, count = lax.axis_index("sp"), lax.axis_size("sp")
    near, far, cross = tp_peers()
    mine = lax.axis_index("tp")
    ahead, behind = peer(sp=(place + 1) % count), peer(sp=(place + count - 1) % count)
    has_left, has_right = place > 0, place < count - 1
    length, width = ref.recept_all.shape
    groups = [slice(g * LANES, (g + 1) * LANES) for g in range(width // LANES)]
    rows = ref.residual.shape[0]
    size = rows // pieces
    mask = block_mask(head_width).astype(jnp.bfloat16)

    weights = Gather(
        (ref.gate, ref.up, ref.down),
        (ref.gates, ref.ups, ref.downs),
        tuple(getattr(ref, name) for name in InnerSems._fields[7:16]),
    )
    shares = Spread(ref.share, ref.shares, ref.share_send, ref.share_recv)
    barrier = pltpu.get_barrier_semaphore()
    for device in (weights.near, weights.far, weights.twin):
        greet(barrier, device)
    pl.semaphore_wait(barrier, 3 + shares.greet(barrier))
    weights.begin()
    loads = [
        pltpu.make_async_copy(source, held, ref.load.at[k])
        for k, (source, held) in enumerate(
            (
                (ref.recept, ref.recept_all),
                (ref.key, ref.key_all),
                (ref.value, ref.value_all),
                (ref.decay, ref.decay_all),
                (ref.rate, ref.rate_all),
                (ref.output_gate, ref.output_gate_all),
                (ref.out_weight, ref.out_weight_all),
                (ref.residual, ref.residual_all),
            )
        )
    ]
    for load in loads:
        load.start()
    for load in loads[:5]:
        load.wait()

    named = ref.route_index[...].astype(jnp.float32).T
    weight = ref.route_weight[...].T
    ids = lax.broadcasted_iota(jnp.int32, ref.share.shape, 1).astype(jnp.float32)
    ref.share[...] = sum(
        jnp.where(named[:, k : k + 1] == ids, weight[:, k : k + 1], 0.0)
        for k in range(named.shape[1])
    )

    full_lanes = lax.broadcasted_iota(jnp.int32, ref.transit.shape, 1) % head_width
    full_rows = lax.broadcasted_iota(jnp.int32, ref.transit.shape, 0)
    ref.transit[...] = jnp.where(full_lanes == full_rows, 1.0, 0.0)
    ref.added[...] = jnp.zeros_like(ref.added)
    chunk_refs = (ref.recept_all, ref.key_all, ref.value_all, ref.decay_all, ref.rate_all, ref.decay_bias, ref.rate_bias)
    per_step = 2

    def chunk_step(step, carry):
        cells, offsets = [], []
        span = per_step * head_width
        by_head = ref.offset[:, pl.ds(pl.multiple_of(step * span, span), span)].T
        for chunk in range(per_step):
            own_offset = by_head[chunk * head_width : (chunk + 1) * head_width]
            offsets += [own_offset] * len(groups)
            first = pl.multiple_of((step * per_step + chunk) * head_width, head_width)
            cells += [(pl.ds(first, head_width), cols) for cols in groups]
        read_map, read_own, low, kept, added, spread = chunk_cells(
            head_width, chunk_refs, cells, offsets
        )
        for k, at in enumerate(cells):
            cols = at[1]
            held_transit, held_added = ref.transit[:, cols], ref.added[:, cols]
            ref.map[at] = single(read_map[k], spread(held_transit), NT).astype(jnp.bfloat16)
            ref.own[at] = read_own[k] + single(read_map[k], spread(held_added), NT)
            held = jnp.concatenate([held_transit, held_added], axis=0)
            moved = held * kept[k] + single(held, low[k])
            ref.transit[:, cols] = moved[:head_width]
            ref.added[:, cols] = moved[head_width:] + added[k]

        for index in range(2):
            pl.when(step == index + 1)(functools.partial(weights.arrive_chip, index))

        return carry

    lax.fori_loop(0, length // (per_step * head_width), chunk_step, 0)

    shares.begin()

    state_ref, onward_ref = ref.state, ref.onward

    def state_copy(group):
        return remote(
            onward_ref.at[group],
            state_ref.at[group],
            ref.state_send.at[group],
            ref.state_recv.at[group],
            ahead,
        )

    @pl.when(place == 0)
    def _():
        for group, cols in enumerate(groups):
            state_ref[group] = jnp.zeros_like(state_ref[group])
            onward_ref[group] = ref.added[:, cols]
            state_copy(group).start()

    weights.arrive_chip(2)

    @pl.when(has_left)
    def _():
        for group, cols in enumerate(groups):
            state_copy(group).wait_recv()

            @pl.when(has_right)
            def _(group=group, cols=cols):
                onward_ref[group] = ref.added[:, cols] + product(
                    halves(state_ref[group]), spread_blocks(ref.transit[:, cols], mask), NN
                )
                state_copy(group).start()

    weights.arrive_chip(3)
    weights.arrive_swap(0)
    weights.arrive_swap(1)
    for load in loads[5:]:
        load.wait()

    mixed_refs = (ref.map, ref.own, ref.recept_all, ref.key_all, ref.value_all, ref.output_gate_all, ref.gain, ref.self_weight)
    core_out, core_in = ref.core_out, ref.core_in
    chip_out, chip_in = ref.chip_out, ref.chip_in

    def partial(owner, part):
        at = pl.ds(pl.multiple_of(owner * rows + part * size, size), size)
        mixed = mixed_rows(head_width, at, state_ref, mixed_refs, mask)
        return single(jnp.concatenate(mixed, axis=1), ref.out_weight_all[...])

    def core_copy(which, part):
        slot = which * pieces + part
        return remote(
            core_out.at[slot],
            core_in.at[slot],
            ref.sum_core_send.at[slot],
            ref.sum_core_recv.at[slot],
            weights.near,
        )

    def chip_copy(part):
        return remote(
            chip_out.at[part],
            chip_in.at[part],
            ref.sum_chip_send.at[part],
            ref.sum_chip_recv.at[part],
            weights.far,
        )

    stream_ref, features_ref = ref.stream, ref.features
    for part in range(pieces):
        core_out[part] = partial(cross, part)
        core_copy(0, part).start()
        own = partial(far, part)
        core_copy(0, part).wait_recv()
        chip_out[part] = (own + core_in[part]).astype(jnp.bfloat16)
        chip_copy(part).start()
        if part == 0:
            weights.begin_late()
    weights.arrive_chip(4)
    weights.arrive_chip(5)

    def sum_own(part):
        at = slice(part * size, (part + 1) * size)
        core_out[pieces + part] = partial(near, part)
        core_copy(1, part).start()
        own = partial(mine, part)
        core_copy(1, part).wait_recv()
        stream_ref[at] = (
            ref.residual_all[at].astype(jnp.float32) + own + core_in[pieces + part]
        )

    def pass_late():
        weights.arrive_swap(4)
        weights.arrive_swap(5)

    def finish_stream(part):
        sum_own(part)
        if part == pieces - 1:
            weights.arrive_chip(LATE)
            weights.arrive_swap(2)
            weights.arrive_swap(3)
        at = slice(part * size, (part + 1) * size)
        chip_copy(part).wait_recv()
        stream = stream_ref[at] + chip_in[part].astype(jnp.float32)
        stream_ref[at] = stream
        features_ref[at] = (
            stream
            * lax.rsqrt(jnp.mean(stream * stream, axis=-1, keepdims=True) + NORM_EPS)
            * ref.norm_gain[...]
        ).astype(jnp.bfloat16)

    def drain_first():
        @pl.when(has_right)
        def _():
            for group in range(len(groups)):
                state_copy(group).wait_send()

        for part in range(pieces):
            core_copy(0, part).wait_send()
            core_copy(1, part).wait_send()
            chip_copy(part).wait_send()
        weights.drain()

    if not with_experts:
        for part in range(pieces):
            finish_stream(part)
        pass_late()
        weights.arrive_rest()
        shares.end()
        drain_first()
        return

    blocks, result, from_right, from_left, to_left, to_right = (getattr(ref, name) for name in Flows._fields)

    def gather_copy(source, block, piece, part, way):
        return remote(
            source,
            blocks.at[block, piece, part],
            ref.gather_send.at[way, block, piece, part],
            ref.gather_recv.at[block, piece, part],
            ahead if way else behind,
        )

    def sum_copy(block, piece, part, way):
        out, into = (to_right, from_left) if way else (to_left, from_right)
        return remote(
            out.at[block, piece, part],
            into.at[block, piece, part],
            ref.flow_send.at[way, block, piece, part],
            ref.flow_recv.at[way, block, piece, part],
            ahead if way else behind,
        )

    parts = blocks.shape[2]
    fine = blocks.shape[3]

    def send_own(piece, way):
        for part in range(parts):
            own_features = features_ref.at[pl.ds(piece * size + part * fine, fine)]
            gather_copy(own_features, place, piece, part, way).start()

    finish_stream(0)
    pl.when(has_left)(lambda: send_own(0, 0))
    pl.when(has_right)(lambda: send_own(0, 1))
    finish_stream(1)
    pl.when(has_left & (place == count - 1))(lambda: send_own(1, 0))
    pl.when(has_right & (place == 0))(lambda: send_own(1, 1))

    def apply(features, block, piece):
        total = None
        for j in range(ref.gates.shape[0]):
            gated = single(features, ref.gates[j])
            upward = single(features, ref.ups[j])
            term = single(jax.nn.silu(gated) * upward, ref.downs[j])
            total = term if total is None else total + term
        own = ref.shares[block, pl.ds(pl.multiple_of(piece * size, size), size)]
        lanes = lax.broadcasted_iota(jnp.int32, own.shape, 1)
        share = jnp.sum(jnp.where(lanes == place, own, 0.0), axis=1, keepdims=True)
        result[block, piece] = (total * share).reshape(parts, fine, total.shape[1])

    def slot(time, carry):
        arrivals = []
        for way, before in ((1, place), (0, count - 1 - place)):
            step = 1 if way else -1
            far = 0 if way else count - 1
            first = time < before
            block = jnp.where(first, place - step * (1 + time), far + step * (time - before))
            piece = jnp.where(first, 0, 1)
            arrivals.append((way, block, piece, time < 2 * before, time == 2 * before - 1))

        for way, block, piece, there, final in arrivals:
            onward = has_right if way else has_left

            @pl.when(there)
            def _(way=way, block=block, piece=piece, onward=onward, final=final):
                for part in range(parts):
                    landed = blocks.at[block, piece, part]
                    gather_copy(landed, block, piece, part, way).wait_recv()
                    pl.when(onward)(
                        lambda: gather_copy(landed, block, piece, part, way).start()
                    )
                pl.when(onward & final)(lambda: send_own(1, way))

        @pl.when(time == 0)
        def _():
            pass_late()
            weights.arrive_rest()
            shares.end()

        own = time - 2 * (count - 1)

        @pl.when((own >= 0) & (own < pieces))
        def _():
            at = pl.ds(pl.multiple_of(own * size, size), size)
            apply(features_ref[at], place, own)

        for way, block, piece, there, final in arrivals:

            @pl.when(there)
            def _(block=block, piece=piece):
                features = blocks[block, piece]
                apply(features.reshape(size, features.shape[2]), block, piece)

        for way, hops, more, into, out in (
            (0, count - 1 - place, has_right, from_right, to_left),
            (1, place, has_left, from_left, to_right),
        ):
            turn = time - lag * hops
            first = turn < count - 1
            offset = jnp.where(first, count - 2 - turn, turn - (count - 1))
            block = count - 1 - offset if way else offset
            piece = jnp.where(first, 0, 1)
            passed = block - place if way else place - block
            valid = (turn >= 0) & (turn < 2 * (count - 1)) & (passed >= 0)

            for part in range(parts):

                @pl.when(valid & more)
                def _(way=way, block=block, piece=piece, part=part, into=into):
                    sum_copy(block, piece, part, way).wait_recv()

                @pl.when(valid & more & (passed > 0))
                def _(block=block, piece=piece, part=part, into=into, out=out):
                    total = result[block, piece, part] + into[block, piece, part].astype(
                        jnp.float32
                    )
                    out[block, piece, part] = total.astype(jnp.bfloat16)

                @pl.when(valid & jnp.logical_not(more))
                def _(block=block, piece=piece, part=part, out=out):
                    out[block, piece, part] = result[block, piece, part].astype(jnp.bfloat16)

                @pl.when(valid & (passed > 0))
                def _(way=way, block=block, piece=piece, part=part):
                    sum_copy(block, piece, part, way).start()

        return carry

    lax.fori_loop(0, (2 + lag) * (count - 1), slot, 0)
    for piece in range(pieces):
        at = slice(piece * size, (piece + 1) * size)
        shape = (size, stream_ref.shape[1])
        stream_ref[at] = stream_ref[at] + result[place, piece].reshape(shape)
        for there, into in ((has_right, from_right), (has_left, from_left)):

            @pl.when(there)
            def _(at=at, into=into, piece=piece):
                stream_ref[at] = stream_ref[at] + into[place, piece].reshape(shape).astype(
                    jnp.float32
                )

        ref.out[at] = stream_ref[at].astype(jnp.bfloat16)

    def drain(block, carry):
        for piece in range(pieces):
            for part in range(parts):
                landed = blocks.at[block, piece, part]
                for way, gathers, sums in (
                    (0, has_left & (block >= place), has_left & (block < place)),
                    (1, has_right & (block <= place), has_right & (block > place)),
                ):
                    pl.when(gathers)(
                        lambda: gather_copy(landed, block, piece, part, way).wait_send()
                    )
                    pl.when(sums)(lambda: sum_copy(block, piece, part, way).wait_send())
        return carry

    lax.fori_loop(0, count, drain, 0)
    drain_first()


def experts_by_collectives(features, stream, shares, gates, ups, downs):
    features = lax.all_gather(features, "sp", axis=0, tiled=True)
    shares = shares.reshape(-1, shares.shape[-1])
    place = lax.axis_index("sp")
    lanes = jnp.arange(shares.shape[1], dtype=jnp.int32)
    share = jnp.sum(jnp.where(lanes[None, :] == place, shares, 0.0), axis=1, keepdims=True)
    depth = features.shape[1]

    def some_rows(operands):
        features, share = operands
        total = None
        for gate, up, down in zip(gates, ups, downs):
            for j in range(gate.shape[0]):
                gated = jnp.dot(features, gate[j], preferred_element_type=jnp.float32)
                upward = jnp.dot(features, up[j], preferred_element_type=jnp.float32)
                hidden = (jax.nn.silu(gated) * upward).astype(jnp.bfloat16)
                term = jnp.dot(hidden, down[j], preferred_element_type=jnp.float32)
                total = term if total is None else total + term
        return (total * share).astype(jnp.bfloat16)

    rows = stream.shape[0]
    total = lax.map(
        some_rows, (features.reshape(-1, rows, depth), share.reshape(-1, rows, 1))
    ).reshape(-1, depth)
    weighted = lax.psum_scatter(total, "sp", scatter_dimension=0, tiled=True)
    return (stream + weighted.astype(jnp.float32)).astype(jnp.bfloat16)


PIECES = 2
PARTS = 2
LAG = 1


def local(
    recept,
    key_input,
    value_input,
    output_gate_input,
    decay_input_part,
    correction_rate_input,
    head_decay_offset,
    decay_fixed_bias,
    correction_rate_bias,
    head_norm_gain,
    self_term_weight,
    output_weight_matrix,
    residual,
    feedforward_norm_gain,
    routed_expert_index,
    routed_expert_weight,
    gate_weight_experts,
    up_weight_experts,
    down_weight_experts,
):
    count = lax.axis_size("sp")
    experts = gate_weight_experts.shape[0] * count
    assert lax.axis_size("tp") == 4 and lax.axis_size("grp") == 2
    assert gate_weight_experts.shape[0] == 1
    length, width = recept.shape
    heads = head_decay_offset.shape[1]
    head_width = width // heads
    own_rows, depth = residual.shape
    shares = jax.ShapeDtypeStruct((residual.shape[0], experts + -experts % 128), jnp.float32)
    gate, up, down = gate_weight_experts[0], up_weight_experts[0], down_weight_experts[0]
    groups = width // LANES
    half = own_rows // PIECES
    dma = pltpu.SemaphoreType.DMA
    single_bf, single_f32 = jnp.bfloat16, jnp.float32

    def like(x):
        return (x.shape, x.dtype)

    kept = dict(
        stream=((own_rows, depth), single_f32),
        features=((own_rows, depth), single_bf),
        shares=((count, *shares.shape), single_f32),
        gates=((4, *gate.shape), gate.dtype),
        ups=((4, *up.shape), up.dtype),
        downs=((4, *down.shape), down.dtype),
    )
    sums = ((2 * PIECES, half, depth), single_f32)
    chips = ((PIECES, half, depth), single_bf)
    states = ((groups, head_width, LANES), single_f32)
    inner = dict(
        recept_all=like(recept),
        key_all=like(key_input),
        value_all=like(value_input),
        decay_all=like(decay_input_part),
        rate_all=like(correction_rate_input),
        output_gate_all=like(output_gate_input),
        out_weight_all=like(output_weight_matrix),
        residual_all=like(residual),
        share=like(shares),
        map=((length, width), single_bf),
        own=((length, width), single_f32),
        transit=((head_width, width), single_f32),
        added=((head_width, width), single_f32),
        state=states,
        onward=states,
        core_out=sums,
        core_in=sums,
        chip_out=chips,
        chip_in=chips,
    )
    sems = [(8,), (groups,), (groups,)] + [(2 * PIECES,)] * 2 + [(PIECES,)] * 2
    portions = len(PORTIONS)
    sems += [(3,)] * 2 + [(portions,)] * 4 + [(2 * portions,)] * 2 + [(3,), (count,), (count,)]
    inner_sems = dict(zip(InnerSems._fields, sems, strict=True))
    with_experts = count <= 4
    scratch, outs = dict(inner), dict(kept)
    if with_experts:
        flow = ((count, PIECES, PARTS, half // PARTS, depth), single_bf)
        scratch = kept | inner
        scratch |= {name: flow for name in Flows._fields} | dict(result=(flow[0], single_f32))
        outs = dict(out=((own_rows, depth), single_bf))
        both = (2, count, PIECES, PARTS)
        inner_sems |= dict(zip(FlowSems._fields, (both, both[1:], both, both), strict=True))
    names = [*Inputs._fields, *outs, *scratch, *inner_sems]
    anywhere = pl.BlockSpec(memory_space=pl.ANY)
    in_vmem = pl.BlockSpec(memory_space=pltpu.VMEM)
    results = pl.pallas_call(
        functools.partial(layer_kernel, names, head_width, PIECES, LAG),
        in_specs=[anywhere] * 5 + [in_vmem] * 8 + [anywhere] * 6,
        out_specs=[in_vmem] * len(outs),
        out_shape=[jax.ShapeDtypeStruct(*spec) for spec in outs.values()],
        scratch_shapes=[pltpu.VMEM(*spec) for spec in scratch.values()]
        + [dma(shape) for shape in inner_sems.values()],
        compiler_params=pltpu.CompilerParams(
            collective_id=0, has_side_effects=True, vmem_limit_bytes=VMEM_LIMIT
        ),
        cost_estimate=pl.CostEstimate(
            flops=30_000_000_000, bytes_accessed=40 * length * width, transcendentals=0
        ),
        name="layer",
    )(
        recept,
        key_input,
        value_input,
        decay_input_part,
        correction_rate_input,
        head_decay_offset.T,
        decay_fixed_bias[None],
        correction_rate_bias[None],
        head_norm_gain[None],
        self_term_weight[None],
        feedforward_norm_gain[None],
        routed_expert_index.T,
        routed_expert_weight.T,
        output_gate_input,
        output_weight_matrix,
        residual,
        gate,
        up,
        down,
    )
    if with_experts:
        return results[0]
    stream, features, all_shares, *full = results
    return experts_by_collectives(features, stream, all_shares, *((each,) for each in full))


def solution(mesh):
    return jax.shard_map(
        local,
        mesh=mesh,
        in_specs=(
            P(("grp", "sp"), "tp"),
            P(("grp", "sp"), "tp"),
            P(("grp", "sp"), "tp"),
            P(("grp", "sp"), "tp"),
            P(("grp", "sp"), "tp"),
            P(("grp", "sp"), "tp"),
            P(("grp", "sp"), "tp"),
            P("tp"),
            P("tp"),
            P("tp"),
            P("tp"),
            P("tp", None),
            P(("grp", "sp", "tp"), None),
            P(),
            P(("grp", "sp", "tp"), None),
            P(("grp", "sp", "tp"), None),
            P("sp", None, "tp"),
            P("sp", None, "tp"),
            P("sp", "tp", None),
        ),
        out_specs=P(("grp", "sp", "tp"), None),
        check_vma=False,
    )
```
